128 devices in a mesh: ep: 16 (over z, x), tp: 8 (over y, core).
Axes of the slice: x: 4, y: 4, z: 4, core: 2. Of those that a mesh axis runs over, the one named last changes fastest.
Arguments:
- queries: bfloat16 [32768, 2048], P('ep', 'tp'), may hold values from -128 to 128
- key_heads: bfloat16 [32768, 1024], P('ep', 'tp'), may hold values from -6 to 6
- value_heads: bfloat16 [32768, 1024], P('ep', 'tp'), may hold values from -6 to 6
- sink_logits: float32 [32], P('tp'), may hold values from 1 to 5
- mix_weight: bfloat16 [2048, 2048], replicated, may hold values from -1 to 1
- expert_input: bfloat16 [16384, 2048], P(('ep', 'tp')), may hold values from -6 to 6
- norm_gain: float32 [2048], replicated, may hold values from 0.1 to 1.9
- routes: int32 [16384, 4], P(('ep', 'tp')), may hold values from 0 to 127, all different within a row; in each aligned block of 128 rows (0 to 127, 128 to 255, ...) at most 8 rows name the same one
- route_weights: float32 [16384, 4], P(('ep', 'tp')), may hold values from 0.1 to 1
- gate_weight: bfloat16 [128, 2048, 1024], P(('ep', 'tp')), may hold values from -0.375 to 0.375
- up_weight: bfloat16 [128, 2048, 1024], P(('ep', 'tp')), may hold values from -0.375 to 0.375
- down_weight: bfloat16 [128, 1024, 2048], P(('ep', 'tp')), may hold values from -0.046875 to 0.046875
Outputs:
- mixer_out: bfloat16 [32768, 2048], P(('ep', 'tp'))
- experts_out: bfloat16 [16384, 2048], P(('ep', 'tp'))
The draws below stay inside these ranges and needn't reach their ends.
Inputs may be any that keep to these rules, and one draw needn't show every extreme that they name: `routes`: each row names 4 different experts; within the 128 rows of one device no expert is named more than 8 times, and in some devices' rows some expert is named exactly 8 times.
All inputs are finite; a program needn't handle non-finite values.
Results may differ from the reference program's by a relative error of at most 0.012.
The reference program's roundings to bfloat16 on the way count: a program that leaves them out, or rounds other values in their place, can miss the bound.
Values may be sent and summed in bfloat16 or wider, within the bound.
A program may use at most 128 MiB of HBM per device.

```python
import math
import jax
import jax.numpy as jnp
import numpy as np
from jax import lax

D = 2048
HEADS = 32
KV_HEADS = 16
HEAD_DIM = 64
WINDOW = 128
GRID_W = 64
FF = 1024
TOPK = 4
TOK_B = 128
TOKENS_A = 32768
TOKENS_B = 16384
EXPERTS = 128
CAP = 8
N_EP = 16
N_TP = 8


def query_key_pair(key):
    base_seed = jax.random.fold_in(key, 7)
    query_seed, key_seed = jax.random.split(base_seed, 2)
    length = TOKENS_A
    key_part = jnp.clip(jax.random.normal(key_seed, (length, KV_HEADS * HEAD_DIM), jnp.float32), -4.0, 4.0)
    query_part = jnp.clip(jax.random.normal(query_seed, (length, HEADS * HEAD_DIM), jnp.float32), -4.0, 4.0)
    return (query_part, key_part)


def draw_queries(key, part):
    return query_key_pair(key)[0].astype(jnp.bfloat16)


def draw_key_heads(key, part):
    return query_key_pair(key)[1].astype(jnp.bfloat16)


def level_of(own_key, extent, pieces, least, top_value):
    gain = 1.0
    for position, blocks in pieces:
        draws = jax.random.uniform(jax.random.fold_in(jax.random.fold_in(own_key, 6), position), (blocks,), jnp.float32, least / len(pieces), top_value / len(pieces))
        gain = gain * jnp.repeat(jnp.exp(draws), extent[position] // blocks).reshape((-1,) + (1,) * (len(extent) - 1 - position))
    return gain


def routed_block(stream_key, own, number, rows, number_of, top, bound, slope):
    sequence = jax.random.permutation(stream_key, number_of)
    heavy_load, usual = shares(number_of, rows * top, bound, slope, True), shares(number_of, rows * top, bound, slope, False)
    places = jnp.arange(number_of)

    def named(lengths, turn):
        used = int((lengths > 0).sum())
        fixed = max(1, used // 4)
        shifted = fixed + (places - fixed + turn * (used - fixed)) % max(1, number_of - fixed)
        return jnp.zeros((number_of,), jnp.int32).at[sequence[jnp.where(places < fixed, places, shifted)]].set(jnp.asarray(lengths, jnp.int32))

    lengths = jnp.where(number % 4 == 0, named(heavy_load, number // 4), named(usual, number - number // 4 - 1))
    mixed = jax.random.permutation(jax.random.fold_in(own, 3), number_of)
    giver, taker = mixed[0:number_of // 2 * 2:2], mixed[1:number_of // 2 * 2:2]
    room = jnp.minimum(lengths[giver] - 1, bound - lengths[taker]) // 2
    room = jnp.where((giver == sequence[0]) | (taker == sequence[0]) | (lengths[taker] == 0), 0, jnp.maximum(room, 0))
    shifted = jax.random.randint(jax.random.fold_in(own, 4), (number_of // 2,), 0, 1 << 20) % (room + 1)
    lengths = lengths.at[giver].add(-shifted).at[taker].add(shifted)
    items = jnp.searchsorted(jnp.cumsum(lengths), jnp.arange(rows * top), side="right").astype(jnp.int32)
    table = items.reshape(top, rows).T
    table = table[jax.random.permutation(jax.random.fold_in(own, 1), rows)]
    turn = jax.random.randint(jax.random.fold_in(own, 2), (rows, 1), 0, top)
    return jnp.take_along_axis(table, (jnp.arange(top)[None, :] + turn) % top, axis=1)


def shares(count, total, most, skew, full):
    loads = [(1 << 20) // math.isqrt(rank ** skew) + 1 for rank in range(1, count + 1)]
    largest = most if full else min(most, max(-(-total // count), total * loads[0] // sum(loads)))
    least = 1 if total - largest >= count - 1 else 0
    counts, rest = [largest] + [least] * (count - 1), total - largest - least * (count - 1)
    while rest > 0:
        candidates = [i for i in range(1, count) if counts[i] < largest] or [i for i in range(1, count) if counts[i] < most]
        whole, budget = sum([loads[i] for i in candidates]), rest
        for i in candidates:
            extra = min(most - counts[i], max(1, budget * loads[i] // whole), rest)
            counts[i] = counts[i] + extra
            rest = rest - extra
    return np.array(counts)


def scatter_about(key, extent, scale, reach, shards=(), kind=jnp.bfloat16):
    result = scale * jax.random.normal(key, extent, jnp.float32)
    if shards:
        result = result * level_of(key, extent, shards, -0.22, 0.18)
    return jnp.clip(result, -reach, reach).astype(kind)


def setup_inputs(seed: int = 0) -> dict:
    key_list = jax.random.split(jax.random.key(seed), 13)
    queries = draw_queries(jax.random.fold_in(key_list[12], 71), 0)
    key_heads = draw_key_heads(jax.random.fold_in(key_list[12], 71), 0)
    value_heads = scatter_about(key_list[2], (TOKENS_A, KV_HEADS * HEAD_DIM), 1.0, 6.0, ((0, 16), (1, 8)))
    sink_logits = jnp.clip(1.0 + 4.0 * jax.random.uniform(key_list[3], (HEADS,), jnp.float32) ** level_of(key_list[3], (HEADS,), ((0, 8),), -0.2, 0.2), 1.0, 5.0)
    mix_weight = scatter_about(key_list[4], (HEADS * HEAD_DIM, D), (HEADS * HEAD_DIM // 64) ** -0.5, 1.0)
    expert_input = scatter_about(key_list[5], (TOKENS_B, D), 1.0, 6.0, ((0, 128),))
    norm_gain = jnp.clip(1.0 + 0.18 * jax.random.normal(key_list[6], (D,), jnp.float32), 0.1, 1.9)
    routes_keys = jax.random.split(jax.random.fold_in(key_list[7], 1), TOKENS_B // TOK_B)
    routes_turns = jax.random.permutation(jax.random.fold_in(key_list[7], 3), TOKENS_B // TOK_B)
    routes = jax.vmap(lambda own, number: routed_block(jax.random.fold_in(key_list[7], 2), own, number, TOK_B, EXPERTS, TOPK, CAP, 2))(routes_keys, routes_turns).reshape((TOKENS_B, TOPK))
    route_weights = jnp.clip(jnp.exp(math.log(1.0) - 2.3025851 * jax.random.uniform(key_list[8], (TOKENS_B, TOPK), jnp.float32) ** level_of(key_list[8], (TOKENS_B, TOPK), ((0, 128),), -0.2, 0.2)), 0.1, 1.0)
    gate_weight = scatter_about(key_list[9], (EXPERTS, D, FF), (D // 9) ** -0.5, 0.375, ((0, 128),))
    up_weight = scatter_about(key_list[10], (EXPERTS, D, FF), (D // 9) ** -0.5, 0.375, ((0, 128),))
    down_weight = scatter_about(key_list[11], (EXPERTS, FF, D), (FF * 16) ** -0.5, 0.046875, ((0, 128),))
    return {"queries": queries, "key_heads": key_heads, "value_heads": value_heads, "sink_logits": sink_logits, "mix_weight": mix_weight, "expert_input": expert_input, "norm_gain": norm_gain, "routes": routes, "route_weights": route_weights, "gate_weight": gate_weight, "up_weight": up_weight, "down_weight": down_weight}


ROPE_BASE = 10000.0
CLAMP_LIMIT = 7.0
GATE_SLOPE = 1.702
NORM_EPS = 1e-05

def rotate_pairs(table, grid_rows, grid_cols, head_width):
    length = table.shape[0]
    quarter = head_width // 4
    shaped = table.reshape(length, -1, 2, 2, quarter)
    freqs = ROPE_BASE ** (-jnp.arange(0, head_width // 2, 2, dtype=jnp.float32) / (head_width // 2))
    angles = jnp.stack([grid_rows, grid_cols], axis=-1)[:, :, None] * freqs
    cosines = jnp.cos(angles)[:, None]
    sine_part = jnp.sin(angles)[:, None]
    former = shaped[..., 0, :]
    latter = shaped[..., 1, :]
    turned = jnp.stack([former * cosines - latter * sine_part, latter * cosines + former * sine_part], axis=-2)
    return turned.reshape(length, -1)

def grid_place(positions):
    return ((positions // GRID_W).astype(jnp.float32), (positions % GRID_W).astype(jnp.float32))

def attend(queries, key_heads, value_heads, sink_logits):
    length = queries.shape[0]
    group_size = HEADS // KV_HEADS
    positions = jnp.arange(length, dtype=jnp.int32)
    grid_rows, grid_cols = grid_place(positions)
    q_rot = rotate_pairs(queries.astype(jnp.float32), grid_rows, grid_cols, HEAD_DIM).astype(jnp.bfloat16)
    k_rot = rotate_pairs(key_heads.astype(jnp.float32), grid_rows, grid_cols, HEAD_DIM).astype(jnp.bfloat16)
    k_padded = jnp.pad(k_rot, ((WINDOW, WINDOW), (0, 0)))
    v_padded = jnp.pad(value_heads, ((WINDOW, WINDOW), (0, 0)))
    block_rows = math.gcd(length, 512)
    key_span = block_rows + 2 * WINDOW
    sink_grid = sink_logits.astype(jnp.float32).reshape(KV_HEADS, group_size)

    def one_block(block_index):
        first_row = block_index * block_rows
        q_blk = lax.dynamic_slice_in_dim(q_rot, first_row, block_rows, 0).astype(jnp.float32)
        q_blk = q_blk.reshape(block_rows, KV_HEADS, group_size, HEAD_DIM)
        k_blk = lax.dynamic_slice_in_dim(k_padded, first_row, key_span, 0).astype(jnp.float32)
        k_blk = k_blk.reshape(key_span, KV_HEADS, HEAD_DIM)
        v_blk = lax.dynamic_slice_in_dim(v_padded, first_row, key_span, 0).astype(jnp.float32)
        v_blk = v_blk.reshape(key_span, KV_HEADS, HEAD_DIM)
        q_pos = first_row + jnp.arange(block_rows, dtype=jnp.int32)
        k_pos = first_row - WINDOW + jnp.arange(key_span, dtype=jnp.int32)
        inside = (jnp.abs(q_pos[:, None] - k_pos[None, :]) <= WINDOW) & (k_pos >= 0) & (k_pos < length)
        scores = jnp.einsum('qkgd,skd->kgqs', q_blk, k_blk) * HEAD_DIM ** (-0.5)
        scores = jnp.where(inside, scores, -jnp.inf)
        peak = jnp.maximum(lax.optimization_barrier(jnp.max(scores, axis=-1)), sink_grid[:, :, None])
        weights_exp = jnp.exp(scores - peak[..., None])
        denominator = lax.optimization_barrier(jnp.sum(weights_exp, axis=-1)) + jnp.exp(sink_grid[:, :, None] - peak)
        chances = (weights_exp / denominator[..., None]).astype(jnp.bfloat16)
        blended = jnp.einsum('kgqs,skd->qkgd', chances.astype(jnp.float32), v_blk)
        return blended.astype(jnp.bfloat16).reshape(block_rows, HEADS * HEAD_DIM)
    blocks = lax.map(one_block, jnp.arange(length // block_rows, dtype=jnp.int32))
    return blocks.reshape(length, HEADS * HEAD_DIM)

def normalize(tokens_in, gain_row):
    values = tokens_in.astype(jnp.float32)
    center = lax.optimization_barrier(jnp.mean(values, axis=-1, keepdims=True))
    spread = lax.optimization_barrier(jnp.mean(jnp.square(values - center), axis=-1, keepdims=True))
    return ((values - center) * lax.rsqrt(spread + NORM_EPS) * gain_row.astype(jnp.float32)).astype(jnp.bfloat16)

def expert_rows(row_block, w_gate, w_lift, w_down):
    gate_pre = jnp.dot(row_block, w_gate, preferred_element_type=jnp.float32)
    lift_pre = jnp.dot(row_block, w_lift, preferred_element_type=jnp.float32)
    gate_pre = jnp.minimum(gate_pre, CLAMP_LIMIT)
    lift_pre = jnp.clip(lift_pre, -CLAMP_LIMIT, CLAMP_LIMIT)
    activated = ((lift_pre + 1.0) * gate_pre * jax.nn.sigmoid(GATE_SLOPE * gate_pre)).astype(jnp.bfloat16)
    return jnp.dot(activated, w_down, preferred_element_type=jnp.float32).astype(jnp.bfloat16)

def slot_within(route_block):
    flat_routes = route_block.reshape(-1)
    matches = (flat_routes[:, None] == jnp.arange(EXPERTS, dtype=jnp.int32)[None, :]).astype(jnp.int32)
    earlier = jnp.cumsum(matches, axis=0) - matches
    return lax.optimization_barrier(jnp.sum(earlier * matches, axis=1)).astype(jnp.int32)

def reference(queries, key_heads, value_heads, sink_logits, mix_weight, expert_input, norm_gain, routes, route_weights, gate_weight, up_weight, down_weight):
    attended = attend(queries, key_heads, value_heads, sink_logits)
    mixer_out = jnp.dot(attended, mix_weight, preferred_element_type=jnp.float32).astype(jnp.bfloat16)
    sources = N_EP * N_TP
    normed = normalize(expert_input, norm_gain)
    slots = jax.vmap(slot_within)(routes.reshape(sources, TOK_B, TOPK)).reshape(-1)
    flat_routes = routes.reshape(-1).astype(jnp.int32)
    token_of = (jnp.arange(TOKENS_B * TOPK, dtype=jnp.int32) // TOPK).astype(jnp.int32)
    source_of = (token_of // TOK_B).astype(jnp.int32)
    columns = (source_of * CAP + slots).astype(jnp.int32)
    table = jnp.full((EXPERTS, sources * CAP), TOKENS_B, jnp.int32).at[flat_routes, columns].set(token_of)
    padded_in = jnp.concatenate([normed, jnp.zeros((1, D), jnp.bfloat16)], axis=0)

    def one_expert(bundle):
        row_ids, w_gate, w_lift, w_down = bundle
        return expert_rows(padded_in[row_ids], w_gate, w_lift, w_down)
    results = lax.map(one_expert, (table, gate_weight, up_weight, down_weight))
    picked = results[flat_routes, columns].reshape(TOKENS_B, TOPK, D)
    summed = lax.optimization_barrier(jnp.sum(route_weights.astype(jnp.float32)[..., None] * picked.astype(jnp.float32), axis=1))
    return (mixer_out, summed.astype(jnp.bfloat16))
```

```python
import functools
import math

import jax
import jax.numpy as jnp
import numpy as np
from jax import lax
from jax.experimental import pallas as pl
from jax.experimental.pallas import tpu as pltpu
from jax.sharding import PartitionSpec as P

MESH = pl.DeviceIdType.MESH
BF16 = jnp.bfloat16
F32 = jnp.float32
GRID_W = 64
ROPE_BASE = 10000.0
CLAMP_LIMIT = 7.0
GATE_SLOPE = 1.702
NORM_EPS = 1e-05
BASE = (0, 1024, 1536)
COLS = (512, 256, 256)
AXES = (0, 1, 2)


def rope_tables():
    freqs = np.float32(ROPE_BASE) ** (-np.arange(0, 32, 2, dtype=np.float32) / np.float32(32))
    lane = np.arange(128)
    by_row = (lane % 64) < 32
    freq = freqs[lane % 16].astype(np.float32)
    rows = np.clip(np.arange(-2, 514), 0, None).astype(np.float32)
    cols = np.arange(64).astype(np.float32)
    row_angle = (rows[:, None] * freq).astype(np.float32).astype(np.float64)
    col_angle = (cols[:, None] * freq).astype(np.float32).astype(np.float64)
    row_cos = np.where(by_row, np.cos(row_angle), 0.0).astype(np.float32)[:, None, :]
    row_sin = np.where(by_row, np.sin(row_angle), 0.0).astype(np.float32)[:, None, :]
    col_cos = np.where(by_row, 0.0, np.cos(col_angle)).astype(np.float32)
    col_sin = np.where(by_row, 0.0, np.sin(col_angle)).astype(np.float32)
    pairs = np.zeros((256, 256), np.float32)
    for l in range(256):
        if l % 32 < 16:
            pairs[l + 16, l] = -1.0
        else:
            pairs[l - 16, l] = 1.0
    return row_cos, row_sin, col_cos, col_sin, pairs


def device(z, x, y, c):
    return (z * 4 + x, y * 2 + c)


def wrap4(v):
    return lax.rem(v, 4)


def aligned(v, n=128):
    return pl.multiple_of(v, n)


def dot(a, b):
    return jnp.dot(a, b, preferred_element_type=F32)


def kernel(
    sink_ref, x_ref, gain_ref, meta_ref, pairs_ref, col_cos_ref, col_sin_ref,
    row_cos_hbm, row_sin_hbm, q_hbm, k_hbm, v_hbm, mix_hbm, wg_hbm, wu_hbm, wd_hbm,
    mo_ref, eo_ref,
    q, kx, vx, krot, kswap, vswap, att, att_in, row_cos, row_sin, mix, wg, wu, wd,
    nrm, metas, ag_y, ag_x, ag_z, pk_y, pk_x, pk_z, arr, act, prod, ret_y, ret_x, ret_z,
    mixing, rs_y, rs_x, rs_z, own_meta, dummy,
    load_sem, halo_send, halo_recv, meta_send, meta_recv, ag_send, ag_recv,
    pk_send, y_recv, x_recv, z_recv, att_send, att_recv, ret_send, ret_recv, rs_send, rs_recv,
):
    ep, tp = lax.axis_index("ep"), lax.axis_index("tp")
    z, x, y, c = ep // 4, lax.rem(ep, 4), tp // 2, lax.rem(tp, 2)
    ag, pk, ret, rs = (ag_y, ag_x, ag_z), (pk_y, pk_x, pk_z), (ret_y, ret_x, ret_z), (rs_y, rs_x, rs_z)

    barrier = pltpu.get_barrier_semaphore()
    peers = 0
    for dz in range(4):
        for dx in range(4):
            for dy in range(4):
                for dc in range(2):
                    if (dz and dx and dy) or not (dz or dx or dy or dc):
                        continue
                    peers += 1
                    pl.semaphore_signal(
                        barrier, 1, device_id=device(wrap4(z + dz), wrap4(x + dx), wrap4(y + dy), c ^ dc),
                        device_id_type=MESH,
                    )

    loads = [
        pltpu.make_async_copy(k_hbm, kx.at[pl.ds(128, 2048)], load_sem.at[0]),
        pltpu.make_async_copy(v_hbm, vx.at[pl.ds(128, 2048)], load_sem.at[1]),
        pltpu.make_async_copy(q_hbm, q, load_sem.at[2]),
        pltpu.make_async_copy(row_cos_hbm.at[pl.ds(ep * 32, 36)], row_cos, load_sem.at[3]),
        pltpu.make_async_copy(row_sin_hbm.at[pl.ds(ep * 32, 36)], row_sin, load_sem.at[4]),
        pltpu.make_async_copy(wg_hbm.at[0], wg, load_sem.at[5]),
        pltpu.make_async_copy(wu_hbm.at[0], wu, load_sem.at[6]),
        pltpu.make_async_copy(wd_hbm.at[0], wd, load_sem.at[7]),
        pltpu.make_async_copy(mix_hbm, mix, load_sem.at[8]),
    ]
    for copy in loads:
        copy.start()

    values = x_ref[...].astype(F32)
    center = jnp.mean(values, axis=-1, keepdims=True)
    moved = values - center
    spread = jnp.mean(jnp.square(moved), axis=-1, keepdims=True)
    nrm[...] = (moved * lax.rsqrt(spread + NORM_EPS) * gain_ref[...]).astype(BF16)
    expert_of = lax.broadcasted_iota(jnp.int32, (128, 128), 0).astype(F32)
    routes = [meta_ref[k : k + 1, :] for k in range(4)]
    named = [(expert_of == routes[k]).astype(F32) for k in range(4)]
    named_any = named[0] + named[1] + named[2] + named[3]
    earlier = (
        lax.broadcasted_iota(jnp.int32, (128, 128), 0) < lax.broadcasted_iota(jnp.int32, (128, 128), 1)
    ).astype(BF16)
    before = dot(named_any.astype(BF16), earlier)
    core = c.astype(F32)
    for k in range(4):
        slot = jnp.sum(before * named[k], axis=0, keepdims=True)
        own_meta[k : k + 1, :] = routes[k] * 16.0 + core * 8.0 + slot
    own_meta[4:8, :] = meta_ref[4:8, :]

    pl.semaphore_wait(barrier, peers)

    def line_peer(axis, j, cc):
        if axis == 0:
            return device(z, x, j, cc)
        if axis == 1:
            return device(z, j, y, cc)
        return device(j, x, y, cc)

    line_pos = (y, x, z)

    def remote(src, dst, ssem, rsem, target):
        pltpu.make_async_remote_copy(
            src_ref=src, dst_ref=dst, send_sem=ssem, recv_sem=rsem, device_id=target, device_id_type=MESH
        ).start()

    def drain(ref, sem):
        pltpu.make_async_copy(ref, ref, sem).wait()

    line_steps = [(0, 1), (1, 0), (1, 1), (3, 0), (3, 1), (2, 0), (2, 1)]
    for axis in AXES:
        for step, dc in line_steps:
            j = wrap4(line_pos[axis] + step)
            remote(
                own_meta, metas.at[axis, line_pos[axis], :, pl.ds(aligned(c * 128), 128)],
                meta_send, meta_recv, line_peer(axis, j, c ^ dc),
            )
    for axis in (2, 1, 0):
        for step, dc in line_steps:
            j = wrap4(line_pos[axis] + step)
            cc = c ^ dc
            first = aligned(BASE[axis] + cc * COLS[axis])
            remote(
                nrm.at[:, pl.ds(first, COLS[axis])], ag[axis].at[line_pos[axis], c],
                ag_send.at[axis], ag_recv.at[axis], line_peer(axis, j, cc),
            )
    after, ahead = lax.rem(ep + 1, 16), lax.rem(ep + 15, 16)
    for n, (src, dst) in enumerate(((k_hbm, kx), (v_hbm, vx))):
        remote(
            src.at[pl.ds(1920, 128)], dst.at[pl.ds(0, 128)], halo_send.at[2 * n], halo_recv.at[2 * n], (after, tp)
        )
        remote(
            src.at[pl.ds(0, 128)], dst.at[pl.ds(2176, 128)], halo_send.at[2 * n + 1], halo_recv.at[2 * n + 1],
            (ahead, tp),
        )
    for axis in AXES:
        first = aligned(BASE[axis] + c * COLS[axis])
        ag[axis][line_pos[axis], c] = nrm[:, pl.ds(first, COLS[axis])]
        metas[axis, line_pos[axis], :, pl.ds(aligned(c * 128), 128)] = own_meta[...]

    def plane_expert(axis, e):
        if axis == 0:
            return (e // 2) * 8 + y * 2 + lax.rem(e, 2)
        if axis == 1:
            return (e // 8) * 32 + x * 8 + lax.rem(e, 8)
        return z * 32 + e

    drain(dummy, meta_recv)
    self_at = ((z * 4 + x) * 2 + c, (z * 4 + y) * 2 + c, (x * 4 + y) * 2 + c)

    def pack(axis):
        drain(ag[axis].at[:, :, pl.ds(0, 112), :], ag_recv.at[axis])
        r = lax.broadcasted_iota(jnp.int32, (512, 256), 0)
        key = (plane_expert(axis, r // 16) * 16 + lax.rem(r, 16)).astype(F32)

        def one(j, carry):
            hit = key == metas[axis, j, 0:1, :]
            for k in range(1, 4):
                hit = hit | (key == metas[axis, j, k : k + 1, :])
            rows = ag[axis][j].reshape(256, COLS[axis])
            packed = dot(hit.astype(F32).astype(BF16), rows).astype(BF16)
            pk[axis][:, j] = packed.reshape(32, 16, COLS[axis])
            return carry

        lax.fori_loop(0, 4, one, 0)

    def cols_of(axis, cc):
        return pl.ds(aligned(BASE[axis] + cc * COLS[axis]), COLS[axis])

    pack(2)
    for dx, dy, dc in [(a, b, d) for a in range(4) for b in range(4) for d in range(2)]:
        xt, yt, ct = wrap4(x + dx), wrap4(y + dy), c ^ dc
        if dx or dy or dc:
            remote(
                pk_z.at[(xt * 4 + yt) * 2 + ct], arr.at[:, x, y, :, cols_of(2, c)],
                pk_send.at[2], z_recv, device(z, xt, yt, ct),
            )
    arr[:, x, y, :, cols_of(2, c)] = pk_z[self_at[2]]
    pack(1)
    for dz, dy, dc in [(a, b, d) for a in range(4) for b in range(4) for d in range(2)]:
        zt, yt, ct = wrap4(z + dz), wrap4(y + dy), c ^ dc
        if dz or dy or dc:
            remote(
                pk_x.at[(zt * 4 + yt) * 2 + ct], arr.at[z, :, y, :, cols_of(1, c)],
                pk_send.at[1], x_recv.at[dz], device(zt, x, yt, ct),
            )
    arr[z, :, y, :, cols_of(1, c)] = pk_x[self_at[1]]
    pack(0)
    for dz, dx, dc in [(a, b, d) for a in range(4) for b in range(4) for d in range(2)]:
        zt, xt, ct = wrap4(z + dz), wrap4(x + dx), c ^ dc
        if dz or dx or dc:
            remote(
                pk_y.at[(zt * 4 + xt) * 2 + ct], arr.at[z, x, :, :, cols_of(0, c)],
                pk_send.at[0], y_recv.at[dz], device(zt, xt, y, ct),
            )
    arr[z, x, :, :, cols_of(0, c)] = pk_y[self_at[0]]

    for copy in loads[:5]:
        copy.wait()
    drain(kx.at[pl.ds(0, 128)], halo_recv.at[0])
    drain(kx.at[pl.ds(2176, 128)], halo_recv.at[1])
    drain(vx.at[pl.ds(0, 128)], halo_recv.at[2])
    drain(vx.at[pl.ds(2176, 128)], halo_recv.at[3])
    low = lax.rem(lax.broadcasted_iota(jnp.int32, (128, 128), 1), 128) < 64

    def turn_tables(g):
        cs = row_cos[pl.ds(g, 2)] + col_cos_ref[...][None]
        sn = row_sin[pl.ds(g, 2)] + col_sin_ref[...][None]
        return cs.reshape(128, 128), sn.reshape(128, 128)

    def turn_keys(b, carry):
        at = pl.ds(aligned(b * 128), 128)
        cs, sn = turn_tables(b * 2)
        kb = kx[at, :]
        turned = kb.astype(F32) * cs + dot(kb, pairs_ref[0:128, 0:128]) * sn
        krot[at, :] = turned.astype(BF16)
        kswap[at, :] = pltpu.roll(turned, 64, 1).astype(BF16)
        vswap[at, :] = pltpu.roll(vx[at, :].astype(F32), 64, 1).astype(BF16)
        return carry

    lax.fori_loop(0, 18, turn_keys, 0)
    i_at = lax.broadcasted_iota(jnp.int32, (256, 128), 0)
    i_at = lax.rem(i_at, 128)
    j_at = lax.broadcasted_iota(jnp.int32, (256, 128), 1)
    gap = j_at - i_at
    upper = lax.broadcasted_iota(jnp.int32, (256, 1), 0) < 128

    def attend(b):
        cs, sn = turn_tables(b * 2 + 2)
        cs = jnp.concatenate([cs, cs], axis=1)
        sn = jnp.concatenate([sn, sn], axis=1)
        qb = q[pl.ds(aligned(b * 128), 128), :]
        qr = (qb.astype(F32) * cs + dot(qb, pairs_ref[...]) * sn) * 0.125
        q01, q23 = qr[:, :128], qr[:, 128:]
        span = pl.ds(aligned(b * 128), 384)
        least = jnp.where((ep == 0) & (b == 0), 1000, 0)
        most = jnp.where((ep == 15) & (b == 15), -1000, 0)

        def pair(q_two, keys, vals, sink):
            s = lax.dot_general(
                q_two.astype(BF16), keys[span, :], (((1,), (1,)), ((), ())), preferred_element_type=F32
            )
            s0 = jnp.where(gap >= least, s[:, :128], -1e30)
            s1 = s[:, 128:256]
            s2 = jnp.where(gap <= most, s[:, 256:], -1e30)
            peak = jnp.maximum(
                jnp.max(jnp.maximum(jnp.maximum(s0, s1), s2), axis=1, keepdims=True), sink
            )
            e0, e1, e2 = jnp.exp(s0 - peak), jnp.exp(s1 - peak), jnp.exp(s2 - peak)
            total = jnp.sum(e0 + e1 + e2, axis=1, keepdims=True) + jnp.exp(sink - peak)
            inv = 1.0 / total
            p = jnp.concatenate([(e * inv).astype(BF16) for e in (e0, e1, e2)], axis=1)
            return dot(p, vals[span, :])

        oa = pair(
            jnp.concatenate([jnp.where(low, q01, 0.0), jnp.where(low, 0.0, q23)], axis=0), krot, vx,
            jnp.where(upper, sink_ref[0], sink_ref[3]),
        )
        ob = pair(
            jnp.concatenate([jnp.where(low, 0.0, q01), jnp.where(low, q23, 0.0)], axis=0), kswap, vswap,
            jnp.where(upper, sink_ref[1], sink_ref[2]),
        )
        out = jnp.concatenate(
            [jnp.where(low, oa[:128], ob[:128]), jnp.where(low, ob[128:], oa[128:])], axis=1
        )
        att[pl.ds(aligned(b * 128), 128), :] = out.astype(BF16)

    def attend_for(s, carry):
        t = lax.rem(tp + 1 + s, 8)

        def half(h, inner):
            attend(t * 2 + h)
            return inner

        lax.fori_loop(0, 2, half, 0)
        here = att.at[pl.ds(aligned(t * 256, 256), 256)]

        @pl.when(s < 7)
        def _():
            remote(here, att_in.at[:, pl.ds(aligned(tp * 256), 256)], att_send, att_recv, (ep, t))

        return carry

    lax.fori_loop(0, 8, attend_for, 0)
    att_in[:, pl.ds(aligned(tp * 256), 256)] = att[pl.ds(aligned(tp * 256, 256), 256), :]

    for axis in AXES:
        r = lax.broadcasted_iota(jnp.int32, (256, 512), 1)
        key = (plane_expert(axis, r // 16) * 16 + lax.rem(r, 16)).astype(F32)

        def weigh(j, carry):
            turned = jnp.transpose(metas[axis, j])
            share = jnp.zeros((256, 512), F32)
            for k in range(4):
                share += jnp.where(key == turned[:, k : k + 1], turned[:, 4 + k : 5 + k], 0.0)
            mixing[axis, j] = share.astype(BF16)
            return carry

        lax.fori_loop(0, 4, weigh, 0)

    for copy in loads[5:8]:
        copy.wait()
    drain(pk_z.at[pl.ds(0, 31)], z_recv)

    for dz in range(4):
        zs = wrap4(z + 4 - dz)
        if dz == 0:
            drain(arr.at[0, :, :, :, pl.ds(0, 896)], y_recv.at[0])
            drain(arr.at[0, pl.ds(0, 2), :, :, pl.ds(0, 896)], x_recv.at[0])
        else:
            drain(arr.at[0, :, :, :, pl.ds(0, 1024)], y_recv.at[dz])
            drain(arr.at[0, :, :, :, pl.ds(0, 512)], x_recv.at[dz])

        def hidden(f, carry):
            at = pl.ds(aligned(f * 256, 256), 256)
            rows = arr[zs].reshape(256, 2048)
            gate = jnp.minimum(dot(rows, wg[:, at]), CLAMP_LIMIT)
            lift = jnp.clip(dot(rows, wu[:, at]), -CLAMP_LIMIT, CLAMP_LIMIT)
            act[:, at] = ((lift + 1.0) * gate * jax.nn.sigmoid(GATE_SLOPE * gate)).astype(BF16)
            return carry

        lax.fori_loop(0, 4, hidden, 0)

        def down(f, carry):
            at = pl.ds(aligned(f * 256, 256), 256)
            res = dot(act[...], wd[:, at]).astype(BF16)
            prod[zs, :, :, :, at] = res.reshape(4, 4, 16, 256)
            return carry

        lax.fori_loop(0, 8, down, 0)

        for d1 in range(4):
            for dc in range(2):
                xt, yt, ct = wrap4(x + d1), wrap4(y + d1), c ^ dc
                if dz or d1 or dc:
                    remote(
                        prod.at[zs, xt, :, :, cols_of(0, ct)], ret_y.at[self_at[0]],
                        ret_send.at[0], ret_recv.at[0], device(zs, xt, y, ct),
                    )
                    remote(
                        prod.at[zs, :, yt, :, cols_of(1, ct)], ret_x.at[self_at[1]],
                        ret_send.at[1], ret_recv.at[1], device(zs, x, yt, ct),
                    )
                else:
                    ret_y[self_at[0]] = prod[zs, x, :, :, cols_of(0, c)]
                    ret_x[self_at[1]] = prod[zs, :, y, :, cols_of(1, c)]
        for dx in range(4):
            for dy in range(4):
                for dc in range(2):
                    xt, yt, ct = wrap4(x + dx), wrap4(y + dy), c ^ dc
                    if dx or dy or dc:
                        remote(
                            prod.at[zs, xt, yt, :, cols_of(2, ct)], ret_z.at[self_at[2], zs],
                            ret_send.at[2], ret_recv.at[2], device(z, xt, yt, ct),
                        )
                    else:
                        ret_z[self_at[2], zs] = prod[zs, x, y, :, cols_of(2, c)]

    loads[8].wait()
    drain(att_in.at[:, pl.ds(0, 1792)], att_recv)

    def project(f, carry):
        at = pl.ds(aligned(f * 256, 256), 256)
        mo_ref[:, at] = dot(att_in[...], mix[:, at]).astype(BF16)
        return carry

    lax.fori_loop(0, 8, project, 0)

    for axis in AXES:
        drain(ag[axis].at[:, :, pl.ds(0, 112), :], ag_send.at[axis])
    for axis in (2, 1, 0):
        drain(ret[axis].at[pl.ds(0, 31)], ret_recv.at[axis])
        for step in (1, 3, 2, 0):
            j = wrap4(line_pos[axis] + step)
            rows = ret[axis][:, j].reshape(512, COLS[axis])
            part = dot(mixing[axis, j], rows).astype(BF16)
            ag[axis][j] = part.reshape(2, 128, COLS[axis])
            slot = (4 - step) % 4
            for dc in range(2):
                cc = c ^ dc
                if step or dc:
                    remote(
                        ag[axis].at[j, cc], rs[axis].at[c, slot],
                        rs_send.at[axis], rs_recv.at[axis], line_peer(axis, j, cc),
                    )
        rs[axis][c, 0] = ag[axis][line_pos[axis], c]
    for axis in (2, 1, 0):
        drain(rs[axis].at[:, :, pl.ds(0, 112), :], rs_recv.at[axis])
        for cc in range(2):
            parts = [rs[axis][cc, s].astype(F32) for s in range(4)]
            first = BASE[axis] + cc * COLS[axis]
            eo_ref[:, first : first + COLS[axis]] = (parts[0] + parts[1] + parts[2] + parts[3]).astype(BF16)

    drain(dummy, meta_send)
    drain(kx.at[pl.ds(0, 128)], halo_send.at[0])
    drain(kx.at[pl.ds(0, 128)], halo_send.at[1])
    drain(kx.at[pl.ds(0, 128)], halo_send.at[2])
    drain(kx.at[pl.ds(0, 128)], halo_send.at[3])
    drain(att_in.at[:, pl.ds(0, 1792)], att_send)
    for axis in AXES:
        drain(pk[axis].at[pl.ds(0, 31)], pk_send.at[axis])
        drain(ret[axis].at[pl.ds(0, 31)], ret_send.at[axis])
        drain(ag[axis].at[:, :, pl.ds(0, 112), :], rs_send.at[axis])


def body(
    queries, key_heads, value_heads, sink_logits, mix_weight, expert_input, norm_gain,
    routes, route_weights, gate_weight, up_weight, down_weight,
):
    row_cos, row_sin, col_cos, col_sin, pairs = rope_tables()
    meta = jnp.concatenate([routes.T.astype(F32), route_weights.T], axis=0)
    vmem = pl.BlockSpec(memory_space=pltpu.VMEM)
    hbm = pl.BlockSpec(memory_space=pl.ANY)
    dma = pltpu.SemaphoreType.DMA
    V = pltpu.VMEM
    scratch = [
        V((2048, 256), BF16), V((2304, 128), BF16), V((2304, 128), BF16),
        V((2304, 128), BF16), V((2304, 128), BF16), V((2304, 128), BF16),
        V((2048, 256), BF16), V((256, 2048), BF16),
        V((36, 1, 128), F32), V((36, 1, 128), F32),
        V((2048, 2048), BF16), V((2048, 1024), BF16), V((2048, 1024), BF16), V((1024, 2048), BF16),
        V((128, 2048), BF16), V((3, 4, 8, 256), F32),
        V((4, 2, 128, 512), BF16), V((4, 2, 128, 256), BF16), V((4, 2, 128, 256), BF16),
        V((32, 4, 16, 512), BF16), V((32, 4, 16, 256), BF16), V((32, 4, 16, 256), BF16),
        V((4, 4, 4, 16, 2048), BF16), V((256, 1024), BF16), V((4, 4, 4, 16, 2048), BF16),
        V((32, 4, 16, 512), BF16), V((32, 4, 16, 256), BF16), V((32, 4, 16, 256), BF16),
        V((3, 4, 256, 512), BF16),
        V((2, 4, 128, 512), BF16), V((2, 4, 128, 256), BF16), V((2, 4, 128, 256), BF16),
        V((8, 128), F32), V((168, 128), F32),
        dma((9,)), dma((4,)), dma((4,)), dma, dma, dma((3,)), dma((3,)),
        dma((3,)), dma((4,)), dma((4,)), dma, dma, dma, dma((3,)), dma((3,)), dma((3,)), dma((3,)),
    ]
    return pl.pallas_call(
        kernel,
        out_shape=(jax.ShapeDtypeStruct((256, 2048), BF16), jax.ShapeDtypeStruct((128, 2048), BF16)),
        in_specs=[pl.BlockSpec(memory_space=pltpu.SMEM)] + [vmem] * 6 + [hbm] * 9,
        out_specs=(vmem, vmem),
        scratch_shapes=scratch,
        compiler_params=pltpu.CompilerParams(
            collective_id=0, has_side_effects=True, vmem_limit_bytes=67043328
        ),
        name="layer",
    )(
        sink_logits, expert_input, norm_gain.reshape(1, -1), meta, jnp.asarray(pairs, BF16),
        jnp.asarray(col_cos), jnp.asarray(col_sin), jnp.asarray(row_cos), jnp.asarray(row_sin),
        queries, key_heads, value_heads, mix_weight, gate_weight, up_weight, down_weight,
    )


def solution(mesh):
    return jax.shard_map(
        body,
        mesh=mesh,
        in_specs=(
            P("ep", "tp"), P("ep", "tp"), P("ep", "tp"), P("tp"), P(), P(("ep", "tp"), None), P(),
            P(("ep", "tp"), None), P(("ep", "tp"), None), P(("ep", "tp"), None, None),
            P(("ep", "tp"), None, None), P(("ep", "tp"), None, None),
        ),
        out_specs=(P(("ep", "tp"), None), P(("ep", "tp"), None)),
        check_vma=False,
    )
```

```python
import random

import jax
import jax.numpy as jnp
import numpy as np
from jax import lax
from jax.experimental import pallas as pl
from jax.experimental.pallas import tpu as pltpu
from jax.sharding import PartitionSpec as P

MESH = pl.DeviceIdType.MESH
BF16 = jnp.bfloat16
F32 = jnp.float32
GRID_W = 64
ROPE_BASE = 10000.0
CLAMP_LIMIT = 7.0
GATE_SLOPE = 1.702
NORM_EPS = 1e-05
BASE = (0, 768, 1536)
COLS = (384, 384, 256)
AXES = (0, 1, 2)
CHUNKS = ((1, 3), (2, 0))


def shuffled(items):
    return random.Random(1).sample(items, len(items))


def messages(chunk, kinds):
    pairs = [(a, b) for a in range(4) for b in range(2)]
    items = []
    for dz in CHUNKS[chunk]:
        for axis in (0, 1):
            if axis in kinds:
                items += [(axis, dz, d, dc) for d, dc in pairs if dz or d or dc]
        if 2 in kinds:
            items += [(2, dz, dx, dy, dc) for dx in range(4) for dy, dc in pairs if dx or dy or dc]
    return shuffled(items)


def rope_tables():
    freqs = np.float32(ROPE_BASE) ** (-np.arange(0, 32, 2, dtype=np.float32) / np.float32(32))
    lane = np.arange(128)
    by_row = (lane % 64) < 32
    freq = freqs[lane % 16].astype(np.float32)
    rows = np.clip(np.arange(-2, 514), 0, None).astype(np.float32)
    cols = np.arange(64).astype(np.float32)
    row_angle = (rows[:, None] * freq).astype(np.float32).astype(np.float64)
    col_angle = (cols[:, None] * freq).astype(np.float32).astype(np.float64)
    row_cos = np.where(by_row, np.cos(row_angle), 0.0).astype(np.float32)[:, None, :]
    row_sin = np.where(by_row, np.sin(row_angle), 0.0).astype(np.float32)[:, None, :]
    col_cos = np.where(by_row, 0.0, np.cos(col_angle)).astype(np.float32)
    col_sin = np.where(by_row, 0.0, np.sin(col_angle)).astype(np.float32)
    pairs = np.zeros((256, 256), np.float32)
    for l in range(256):
        if l % 32 < 16:
            pairs[l + 16, l] = -1.0
        else:
            pairs[l - 16, l] = 1.0
    return row_cos, row_sin, col_cos, col_sin, pairs


def device(z, x, y, c):
    return (z * 4 + x, y * 2 + c)


def wrap4(v):
    return lax.rem(v, 4)


def aligned(v, n=128):
    return pl.multiple_of(v, n)


def dot(a, b):
    return jnp.dot(a, b, preferred_element_type=F32)


def kernel(
    sink_ref, x_ref, gain_ref, routes_ref, shares_ref, pairs_ref, col_cos_ref, col_sin_ref,
    row_cos_hbm, row_sin_hbm, q_hbm, k_hbm, v_hbm, mix_hbm, wg_hbm, wu_hbm, wd_hbm,
    mo_ref, eo_ref,
    q, kx, vx, krot, kswap, vswap, att, att_in, row_cos, row_sin, mix, wg, wu, wd,
    nrm, metas, ag_y, ag_x, ag_z, pk_y, pk_x, pk_z, arr, act, prod, ret_y, ret_x, ret_z,
    mixing, rs_y, rs_x, rs_z, own_meta, dummy,
    load_sem, halo_send, halo_recv, meta_send, meta_recv, ag_send, ag_recv,
    pk_send, row_recv, att_send, att_recv, ret_send, ret_recv, rs_send, rs_recv,
):
    ep, tp = lax.axis_index("ep"), lax.axis_index("tp")
    z, x, y, c = ep // 4, lax.rem(ep, 4), tp // 2, lax.rem(tp, 2)
    ag, pk, ret, rs = (ag_y, ag_x, ag_z), (pk_y, pk_x, pk_z), (ret_y, ret_x, ret_z), (rs_y, rs_x, rs_z)

    barrier = pltpu.get_barrier_semaphore()
    peers = 0
    for dz in range(4):
        for dx in range(4):
            for dy in range(4):
                for dc in range(2):
                    if (dz and dx and dy) or not (dz or dx or dy or dc):
                        continue
                    peers += 1
                    pl.semaphore_signal(
                        barrier, 1, device_id=device(wrap4(z + dz), wrap4(x + dx), wrap4(y + dy), c ^ dc),
                        device_id_type=MESH,
                    )

    loads = [
        pltpu.make_async_copy(k_hbm, kx.at[pl.ds(128, 2048)], load_sem.at[0]),
        pltpu.make_async_copy(v_hbm, vx.at[pl.ds(128, 2048)], load_sem.at[1]),
        pltpu.make_async_copy(q_hbm, q, load_sem.at[2]),
        pltpu.make_async_copy(row_cos_hbm.at[pl.ds(ep * 32, 36)], row_cos, load_sem.at[3]),
        pltpu.make_async_copy(row_sin_hbm.at[pl.ds(ep * 32, 36)], row_sin, load_sem.at[4]),
        pltpu.make_async_copy(wg_hbm.at[0], wg, load_sem.at[5]),
        pltpu.make_async_copy(wu_hbm.at[0], wu, load_sem.at[6]),
        pltpu.make_async_copy(wd_hbm.at[0], wd, load_sem.at[7]),
        pltpu.make_async_copy(mix_hbm, mix, load_sem.at[8]),
    ]
    for copy in loads:
        copy.start()

    values = x_ref[...].astype(F32)
    center = jnp.mean(values, axis=-1, keepdims=True)
    moved = values - center
    spread = jnp.mean(jnp.square(moved), axis=-1, keepdims=True)
    nrm[...] = (moved * lax.rsqrt(spread + NORM_EPS) * gain_ref[...]).astype(BF16)
    expert_of = lax.broadcasted_iota(jnp.int32, (128, 128), 0).astype(F32)
    routes = [routes_ref[k : k + 1, :].astype(F32) for k in range(4)]
    named = [(expert_of == routes[k]).astype(F32) for k in range(4)]
    named_any = named[0] + named[1] + named[2] + named[3]
    earlier = (
        lax.broadcasted_iota(jnp.int32, (128, 128), 0) < lax.broadcasted_iota(jnp.int32, (128, 128), 1)
    ).astype(BF16)
    before = dot(named_any.astype(BF16), earlier)
    core = c.astype(F32)
    for k in range(4):
        slot = jnp.sum(before * named[k], axis=0, keepdims=True)
        own_meta[k : k + 1, :] = routes[k] * 16.0 + core * 8.0 + slot
        own_meta[4 + k : 5 + k, :] = shares_ref[k : k + 1, :]

    pl.semaphore_wait(barrier, peers)

    def line_peer(axis, j, cc):
        if axis == 0:
            return device(z, x, j, cc)
        if axis == 1:
            return device(z, j, y, cc)
        return device(j, x, y, cc)

    line_pos = (y, x, z)

    def remote(src, dst, ssem, rsem, target):
        pltpu.make_async_remote_copy(
            src_ref=src, dst_ref=dst, send_sem=ssem, recv_sem=rsem, device_id=target, device_id_type=MESH
        ).start()

    def drain(ref, sem):
        pltpu.make_async_copy(ref, ref, sem).wait()

    line_steps = [(0, 1), (1, 0), (1, 1), (3, 0), (3, 1), (2, 0), (2, 1)]
    for axis in AXES:
        for step, dc in line_steps:
            j = wrap4(line_pos[axis] + step)
            remote(
                own_meta, metas.at[axis, line_pos[axis], :, pl.ds(aligned(c * 128), 128)],
                meta_send, meta_recv, line_peer(axis, j, c ^ dc),
            )
    for axis in (2, 1, 0):
        for step, dc in line_steps:
            j = wrap4(line_pos[axis] + step)
            cc = c ^ dc
            first = aligned(BASE[axis] + cc * COLS[axis])
            remote(
                nrm.at[:, pl.ds(first, COLS[axis])], ag[axis].at[line_pos[axis], c],
                ag_send.at[axis], ag_recv.at[axis], line_peer(axis, j, cc),
            )
    after, ahead = lax.rem(ep + 1, 16), lax.rem(ep + 15, 16)
    for n, (src, dst) in enumerate(((k_hbm, kx), (v_hbm, vx))):
        remote(
            src.at[pl.ds(1920, 128)], dst.at[pl.ds(0, 128)], halo_send.at[2 * n], halo_recv.at[2 * n], (after, tp)
        )
        remote(
            src.at[pl.ds(0, 128)], dst.at[pl.ds(2176, 128)], halo_send.at[2 * n + 1], halo_recv.at[2 * n + 1],
            (ahead, tp),
        )
    for axis in AXES:
        first = aligned(BASE[axis] + c * COLS[axis])
        ag[axis][line_pos[axis], c] = nrm[:, pl.ds(first, COLS[axis])]
        metas[axis, line_pos[axis], :, pl.ds(aligned(c * 128), 128)] = own_meta[...]

    def plane_expert(axis, e):
        if axis == 0:
            return (e // 2) * 8 + y * 2 + lax.rem(e, 2)
        if axis == 1:
            return (e // 8) * 32 + x * 8 + lax.rem(e, 8)
        return z * 32 + e

    self_at = ((z * 4 + x) * 2 + c, (z * 4 + y) * 2 + c, (x * 4 + y) * 2 + c)

    def pack(axis):
        drain(ag[axis].at[:, :, pl.ds(0, 112), :], ag_recv.at[axis])
        r = lax.broadcasted_iota(jnp.int32, (512, 256), 0)
        key = (plane_expert(axis, r // 16) * 16 + lax.rem(r, 16)).astype(F32)

        def one(j, carry):
            hit = key == metas[axis, j, 0:1, :]
            for k in range(1, 4):
                hit = hit | (key == metas[axis, j, k : k + 1, :])
            rows = ag[axis][j].reshape(256, COLS[axis])
            packed = dot(hit.astype(F32).astype(BF16), rows).astype(BF16)
            pk[axis][:, j] = packed.reshape(32, 16, COLS[axis])
            return carry

        lax.fori_loop(0, 4, one, 0)

    def cols_of(axis, cc):
        return pl.ds(aligned(BASE[axis] + cc * COLS[axis]), COLS[axis])

    def weigh_axis(axis):
        r = lax.broadcasted_iota(jnp.int32, (256, 512), 1)
        key = (plane_expert(axis, r // 16) * 16 + lax.rem(r, 16)).astype(F32)

        def weigh(j, carry):
            turned = jnp.transpose(metas[axis, j])
            share = jnp.zeros((256, 512), F32)
            for k in range(4):
                share += jnp.where(key == turned[:, k : k + 1], turned[:, 4 + k : 5 + k], 0.0)
            mixing[axis, j] = share.astype(BF16)
            return carry

        lax.fori_loop(0, 4, weigh, 0)

    for copy in loads[:5]:
        copy.wait()
    low = lax.rem(lax.broadcasted_iota(jnp.int32, (128, 128), 1), 128) < 64

    def turn_tables(g):
        cs = row_cos[pl.ds(g, 2)] + col_cos_ref[...][None]
        sn = row_sin[pl.ds(g, 2)] + col_sin_ref[...][None]
        return cs.reshape(128, 128), sn.reshape(128, 128)

    def turn_keys(b, carry):
        at = pl.ds(aligned(b * 128), 128)
        cs, sn = turn_tables(b * 2)
        kb = kx[at, :]
        turned = kb.astype(F32) * cs + dot(kb, pairs_ref[0:128, 0:128]) * sn
        krot[at, :] = turned.astype(BF16)
        kswap[at, :] = pltpu.roll(turned, 64, 1).astype(BF16)
        vswap[at, :] = pltpu.roll(vx[at, :].astype(F32), 64, 1).astype(BF16)
        return carry

    lax.fori_loop(1, 17, turn_keys, 0)
    i_at = lax.broadcasted_iota(jnp.int32, (256, 128), 0)
    i_at = lax.rem(i_at, 128)
    j_at = lax.broadcasted_iota(jnp.int32, (256, 128), 1)
    gap = j_at - i_at
    upper = lax.broadcasted_iota(jnp.int32, (256, 1), 0) < 128

    def attend(b):
        cs, sn = turn_tables(b * 2 + 2)
        cs = jnp.concatenate([cs, cs], axis=1)
        sn = jnp.concatenate([sn, sn], axis=1)
        qb = q[pl.ds(aligned(b * 128), 128), :]
        qr = (qb.astype(F32) * cs + dot(qb, pairs_ref[...]) * sn) * 0.125
        q01, q23 = qr[:, :128], qr[:, 128:]
        span = pl.ds(aligned(b * 128), 384)
        least = jnp.where((ep == 0) & (b == 0), 1000, 0)
        most = jnp.where((ep == 15) & (b == 15), -1000, 0)

        def pair(q_two, keys, vals, sink):
            s = lax.dot_general(
                q_two.astype(BF16), keys[span, :], (((1,), (1,)), ((), ())), preferred_element_type=F32
            )
            s0 = jnp.where(gap >= least, s[:, :128], -1e30)
            s1 = s[:, 128:256]
            s2 = jnp.where(gap <= most, s[:, 256:], -1e30)
            peak = jnp.maximum(
                jnp.max(jnp.maximum(jnp.maximum(s0, s1), s2), axis=1, keepdims=True), sink
            )
            e0, e1, e2 = jnp.exp(s0 - peak), jnp.exp(s1 - peak), jnp.exp(s2 - peak)
            total = jnp.sum(e0 + e1 + e2, axis=1, keepdims=True) + jnp.exp(sink - peak)
            inv = 1.0 / total
            p = jnp.concatenate([(e * inv).astype(BF16) for e in (e0, e1, e2)], axis=1)
            return dot(p, vals[span, :])

        oa = pair(
            jnp.concatenate([jnp.where(low, q01, 0.0), jnp.where(low, 0.0, q23)], axis=0), krot, vx,
            jnp.where(upper, sink_ref[0], sink_ref[3]),
        )
        ob = pair(
            jnp.concatenate([jnp.where(low, 0.0, q01), jnp.where(low, q23, 0.0)], axis=0), kswap, vswap,
            jnp.where(upper, sink_ref[1], sink_ref[2]),
        )
        out = jnp.concatenate(
            [jnp.where(low, oa[:128], ob[:128]), jnp.where(low, ob[128:], oa[128:])], axis=1
        )
        att[pl.ds(aligned(b * 128), 128), :] = out.astype(BF16)

    def attend_for(s, carry):
        t = lax.rem(tp + 1 + s, 8)

        def half(h, inner):
            attend(t * 2 + h)
            return inner

        lax.fori_loop(0, 2, half, 0)
        here = att.at[pl.ds(aligned(t * 256, 256), 256)]

        @pl.when(s < 7)
        def _():
            remote(here, att_in.at[:, pl.ds(aligned(tp * 256), 256)], att_send, att_recv, (ep, t))

        return carry

    drain(dummy, meta_recv)
    weigh_axis(2)
    weigh_axis(1)
    def send_rows(items):
        for axis, dz, *rest in items:
            if axis == 0:
                zt, xt, ct = wrap4(z + dz), wrap4(x + rest[0]), c ^ rest[1]
                src, dst = pk_y.at[(zt * 4 + xt) * 2 + ct], arr.at[z, x, :, :, cols_of(0, c)]
                target = device(zt, xt, y, ct)
            elif axis == 1:
                zt, yt, ct = wrap4(z + dz), wrap4(y + rest[0]), c ^ rest[1]
                src, dst = pk_x.at[(zt * 4 + yt) * 2 + ct], arr.at[z, :, y, :, cols_of(1, c)]
                target = device(zt, x, yt, ct)
            else:
                xt, yt, ct = wrap4(x + rest[0]), wrap4(y + rest[1]), c ^ rest[2]
                zs = wrap4(z + 4 - dz)
                src, dst = pk_z.at[(xt * 4 + yt) * 2 + ct, zs], arr.at[zs, x, y, :, cols_of(2, c)]
                target = device(z, xt, yt, ct)
            chunk = 0 if dz in CHUNKS[0] else 1
            remote(src, dst, pk_send.at[axis], row_recv.at[axis, chunk], target)

    pack(2)
    send_rows(messages(0, (2,)))
    pack(1)
    pack(0)
    send_rows(messages(0, (0, 1)))
    arr[:, x, y, :, cols_of(2, c)] = pk_z[self_at[2]]
    arr[z, :, y, :, cols_of(1, c)] = pk_x[self_at[1]]
    arr[z, x, :, :, cols_of(0, c)] = pk_y[self_at[0]]

    drain(kx.at[pl.ds(0, 128)], halo_recv.at[0])
    drain(kx.at[pl.ds(2176, 128)], halo_recv.at[1])
    drain(vx.at[pl.ds(0, 128)], halo_recv.at[2])
    drain(vx.at[pl.ds(2176, 128)], halo_recv.at[3])
    turn_keys(0, 0)
    turn_keys(17, 0)
    lax.fori_loop(0, 3, attend_for, 0)
    send_rows(messages(1, (0, 1, 2)))
    lax.fori_loop(3, 8, attend_for, 0)
    weigh_axis(0)
    att_in[:, pl.ds(aligned(tp * 256), 256)] = att[pl.ds(aligned(tp * 256, 256), 256), :]

    for copy in loads[5:8]:
        copy.wait()
    for chunk in range(2):
        drain(pk_y.at[pl.ds(0, 16 - chunk)], row_recv.at[0, chunk])
        drain(pk_x.at[pl.ds(0, 16 - chunk)], row_recv.at[1, chunk])
        drain(pk_z.at[pl.ds(0, 31), pl.ds(0, 2)], row_recv.at[2, chunk])
        z0, z1 = [wrap4(z + 4 - dz) for dz in CHUNKS[chunk]]

        def hidden(f, carry):
            at = pl.ds(aligned(f * 256, 256), 256)
            rows = jnp.concatenate([arr[z0].reshape(256, 2048), arr[z1].reshape(256, 2048)], axis=0)
            gate = jnp.minimum(dot(rows, wg[:, at]), CLAMP_LIMIT)
            lift = jnp.clip(dot(rows, wu[:, at]), -CLAMP_LIMIT, CLAMP_LIMIT)
            act[:, at] = ((lift + 1.0) * gate * jax.nn.sigmoid(GATE_SLOPE * gate)).astype(BF16)
            return carry

        lax.fori_loop(0, 4, hidden, 0)

        def down(f, carry):
            at = pl.ds(aligned(f * 256, 256), 256)
            res = dot(act[...], wd[:, at]).astype(BF16)
            prod[z0, :, :, :, at] = res[:256].reshape(4, 4, 16, 256)
            prod[z1, :, :, :, at] = res[256:].reshape(4, 4, 16, 256)
            return carry

        lax.fori_loop(0, 8, down, 0)

        for axis, dz, *rest in messages(chunk, (0, 1, 2)):
            zs = wrap4(z + 4 - dz)
            if axis == 0:
                xt, ct = wrap4(x + rest[0]), c ^ rest[1]
                src, dst = prod.at[zs, xt, :, :, cols_of(0, ct)], ret_y.at[self_at[0]]
                target = device(zs, xt, y, ct)
            elif axis == 1:
                yt, ct = wrap4(y + rest[0]), c ^ rest[1]
                src, dst = prod.at[zs, :, yt, :, cols_of(1, ct)], ret_x.at[self_at[1]]
                target = device(zs, x, yt, ct)
            else:
                xt, yt, ct = wrap4(x + rest[0]), wrap4(y + rest[1]), c ^ rest[2]
                src, dst = prod.at[zs, xt, yt, :, cols_of(2, ct)], ret_z.at[self_at[2], zs]
                target = device(z, xt, yt, ct)
            remote(src, dst, ret_send.at[axis], ret_recv.at[axis], target)
        if chunk == 1:
            ret_y[self_at[0]] = prod[z, x, :, :, cols_of(0, c)]
            ret_x[self_at[1]] = prod[z, :, y, :, cols_of(1, c)]
        for zs in (z0, z1):
            ret_z[self_at[2], zs] = prod[zs, x, y, :, cols_of(2, c)]

    loads[8].wait()
    drain(att_in.at[:, pl.ds(0, 1792)], att_recv)

    def project(f, carry):
        at = pl.ds(aligned(f * 256, 256), 256)
        mo_ref[:, at] = dot(att_in[...], mix[:, at]).astype(BF16)
        return carry

    lax.fori_loop(0, 8, project, 0)

    for axis in AXES:
        drain(ag[axis].at[:, :, pl.ds(0, 112), :], ag_send.at[axis])
    for axis in (2, 1, 0):
        drain(ret[axis].at[pl.ds(0, 31)], ret_recv.at[axis])
        for step in (1, 3, 2, 0):
            j = wrap4(line_pos[axis] + step)
            rows = ret[axis][:, j].reshape(512, COLS[axis])
            part = dot(mixing[axis, j], rows).astype(BF16)
            ag[axis][j] = part.reshape(2, 128, COLS[axis])
            slot = (4 - step) % 4
            for dc in range(2):
                cc = c ^ dc
                if step or dc:
                    remote(
                        ag[axis].at[j, cc], rs[axis].at[c, slot],
                        rs_send.at[axis], rs_recv.at[axis], line_peer(axis, j, cc),
                    )
        rs[axis][c, 0] = ag[axis][line_pos[axis], c]
    for axis in (2, 1, 0):
        drain(rs[axis].at[:, :, pl.ds(0, 112), :], rs_recv.at[axis])
        for cc in range(2):
            parts = [rs[axis][cc, s].astype(F32) for s in range(4)]
            first = BASE[axis] + cc * COLS[axis]
            eo_ref[:, first : first + COLS[axis]] = (parts[0] + parts[1] + parts[2] + parts[3]).astype(BF16)

    drain(dummy, meta_send)
    drain(kx.at[pl.ds(0, 128)], halo_send.at[0])
    drain(kx.at[pl.ds(0, 128)], halo_send.at[1])
    drain(kx.at[pl.ds(0, 128)], halo_send.at[2])
    drain(kx.at[pl.ds(0, 128)], halo_send.at[3])
    drain(att_in.at[:, pl.ds(0, 1792)], att_send)
    for axis in AXES:
        drain(pk[axis].at[pl.ds(0, 31)], pk_send.at[axis])
        drain(ret[axis].at[pl.ds(0, 31)], ret_send.at[axis])
        drain(ag[axis].at[:, :, pl.ds(0, 112), :], rs_send.at[axis])


def body(
    queries, key_heads, value_heads, sink_logits, mix_weight, expert_input, norm_gain,
    routes, route_weights, gate_weight, up_weight, down_weight,
):
    row_cos, row_sin, col_cos, col_sin, pairs = rope_tables()
    vmem = pl.BlockSpec(memory_space=pltpu.VMEM)
    hbm = pl.BlockSpec(memory_space=pl.ANY)
    dma = pltpu.SemaphoreType.DMA
    V = pltpu.VMEM
    scratch = [
        V((2048, 256), BF16), V((2304, 128), BF16), V((2304, 128), BF16),
        V((2304, 128), BF16), V((2304, 128), BF16), V((2304, 128), BF16),
        V((2048, 256), BF16), V((256, 2048), BF16),
        V((36, 1, 128), F32), V((36, 1, 128), F32),
        V((2048, 2048), BF16), V((2048, 1024), BF16), V((2048, 1024), BF16), V((1024, 2048), BF16),
        V((128, 2048), BF16), V((3, 4, 8, 256), F32),
        *[V((4, 2, 128, n), BF16) for n in COLS],
        *[V((32, 4, 16, n), BF16) for n in COLS],
        V((4, 4, 4, 16, 2048), BF16), V((512, 1024), BF16), V((4, 4, 4, 16, 2048), BF16),
        *[V((32, 4, 16, n), BF16) for n in COLS],
        V((3, 4, 256, 512), BF16),
        *[V((2, 4, 128, n), BF16) for n in COLS],
        V((8, 128), F32), V((168, 128), F32),
        dma((9,)), dma((4,)), dma((4,)), dma, dma, dma((3,)), dma((3,)),
        dma((3,)), dma((3, 2)), dma, dma, dma((3,)), dma((3,)), dma((3,)), dma((3,)),
    ]
    mixed, summed = pl.pallas_call(
        kernel,
        out_shape=(jax.ShapeDtypeStruct((256, 2048), BF16), jax.ShapeDtypeStruct((128, 2048), BF16)),
        in_specs=[pl.BlockSpec(memory_space=pltpu.SMEM)] + [vmem] * 7 + [hbm] * 9,
        out_specs=(vmem, vmem),
        scratch_shapes=scratch,
        compiler_params=pltpu.CompilerParams(
            collective_id=0, has_side_effects=True, vmem_limit_bytes=67043328
        ),
        name="layer",
    )(
        sink_logits, expert_input, norm_gain.reshape(1, -1), routes.T, route_weights.T, jnp.asarray(pairs, BF16),
        jnp.asarray(col_cos), jnp.asarray(col_sin), jnp.asarray(row_cos), jnp.asarray(row_sin),
        queries, key_heads, value_heads, mix_weight, gate_weight, up_weight, down_weight,
    )
    return pl.pallas_call(
        hand_over,
        out_shape=(jax.ShapeDtypeStruct((256, 2048), BF16), jax.ShapeDtypeStruct((128, 2048), BF16)),
        in_specs=[hbm] * 2,
        out_specs=(hbm, hbm),
        scratch_shapes=[V((384, 2048), BF16), dma((3,)), dma((3,))],
        name="finish",
    )(mixed, summed)


def hand_over(mixed, summed, mixed_out, summed_out, held, in_sem, out_sem):
    parts = [(mixed, mixed_out, 0, 0), (mixed, mixed_out, 128, 128), (summed, summed_out, 0, 256)]
    takes, gives = [], []
    for n, (src, dst, first, at) in enumerate(parts):
        here = held.at[pl.ds(at, 128)]
        takes.append(pltpu.make_async_copy(src.at[pl.ds(first, 128)], here, in_sem.at[n]))
        gives.append(pltpu.make_async_copy(here, dst.at[pl.ds(first, 128)], out_sem.at[n]))
    for copy in takes:
        copy.start()
    for take, give in zip(takes, gives):
        take.wait()
        give.start()
    for copy in gives:
        copy.wait()


def solution(mesh):
    return jax.shard_map(
        body,
        mesh=mesh,
        in_specs=(
            P("ep", "tp"), P("ep", "tp"), P("ep", "tp"), P("tp"), P(), P(("ep", "tp"), None), P(),
            P(("ep", "tp"), None), P(("ep", "tp"), None), P(("ep", "tp"), None, None),
            P(("ep", "tp"), None, None), P(("ep", "tp"), None, None),
        ),
        out_specs=(P(("ep", "tp"), None), P(("ep", "tp"), None)),
        check_vma=False,
    )
```

```python
import random

import jax
import jax.numpy as jnp
import numpy as np
from jax import lax
from jax.experimental import pallas as pl
from jax.experimental.pallas import tpu as pltpu
from jax.sharding import PartitionSpec as P

MESH = pl.DeviceIdType.MESH
BF16 = jnp.bfloat16
F32 = jnp.float32
GRID_W = 64
ROPE_BASE = 10000.0
CLAMP_LIMIT = 7.0
GATE_SLOPE = 1.702
NORM_EPS = 1e-05
BASE = (0, 768, 1536)
COLS = (384, 384, 256)
BACK_BASE = (0, 768, 1536)
BACK_COLS = (384, 384, 256)
AXES = (0, 1, 2)
CHUNKS = ((1, 3), (2, 0))


def shuffled(items):
    return random.Random(1).sample(items, len(items))


def messages(chunk, kinds):
    pairs = [(a, b) for a in range(4) for b in range(2)]
    items = []
    for dz in CHUNKS[chunk]:
        for axis in (0, 1):
            if axis in kinds:
                items += [(axis, dz, d, dc, n) for d, dc in pairs if dz or d or dc for n in range(4)]
        if 2 in kinds:
            items += [(2, dz, dx, dy, dc) for dx in range(4) for dy, dc in pairs if dx or dy or dc]
    return shuffled(items)


def rope_tables():
    freqs = np.float32(ROPE_BASE) ** (-np.arange(0, 32, 2, dtype=np.float32) / np.float32(32))
    lane = np.arange(128)
    by_row = (lane % 64) < 32
    freq = freqs[lane % 16].astype(np.float32)
    rows = np.clip(np.arange(-2, 514), 0, None).astype(np.float32)
    cols = np.arange(64).astype(np.float32)
    row_angle = (rows[:, None] * freq).astype(np.float32).astype(np.float64)
    col_angle = (cols[:, None] * freq).astype(np.float32).astype(np.float64)
    row_cos = np.where(by_row, np.cos(row_angle), 0.0).astype(np.float32)[:, None, :]
    row_sin = np.where(by_row, np.sin(row_angle), 0.0).astype(np.float32)[:, None, :]
    col_cos = np.where(by_row, 0.0, np.cos(col_angle)).astype(np.float32)
    col_sin = np.where(by_row, 0.0, np.sin(col_angle)).astype(np.float32)
    pairs = np.zeros((256, 256), np.float32)
    for l in range(256):
        if l % 32 < 16:
            pairs[l + 16, l] = -1.0
        else:
            pairs[l - 16, l] = 1.0
    return row_cos, row_sin, col_cos, col_sin, pairs


def device(z, x, y, c):
    return (z * 4 + x, y * 2 + c)


def wrap4(v):
    return lax.rem(v, 4)


def aligned(v, n=128):
    return pl.multiple_of(v, n)


def dot(a, b):
    return jnp.dot(a, b, preferred_element_type=F32)


def kernel(
    sink_ref, x_hbm, gain_hbm, routes_hbm, shares_hbm, pairs_hbm, col_cos_hbm, col_sin_hbm,
    row_cos_hbm, row_sin_hbm, q_hbm, k_hbm, v_hbm, mix_hbm, wg_hbm, wu_hbm, wd_hbm,
    mo_hbm, eo_hbm,
    x_ref, gain_ref, routes_ref, shares_ref, pairs_ref, col_cos_ref, col_sin_ref, mo_ref, eo_ref, give_sem, q, kx, vx, krot, kswap, vswap, att, att_in, row_cos, row_sin, mix, wg, wu, wd,
    nrm, metas, ag_y, ag_x, ag_z, pk_y, pk_x, pk_z, arr, act, prod, ret_y, ret_x, ret_z,
    mixing, picks, rs_y, rs_x, rs_z, out_y, out_x, out_z, own_meta, dummy,
    load_sem, halo_send, halo_recv, meta_send, meta_recv, ag_send, ag_recv,
    pk_send, row_recv, att_send, att_recv, ret_send, ret_recv, rs_send, rs_recv,
):
    ep, tp = lax.axis_index("ep"), lax.axis_index("tp")
    z, x, y, c = ep // 4, lax.rem(ep, 4), tp // 2, lax.rem(tp, 2)
    ag, pk, ret, rs = (ag_y, ag_x, ag_z), (pk_y, pk_x, pk_z), (ret_y, ret_x, ret_z), (rs_y, rs_x, rs_z)
    out = (out_y, out_x, out_z)

    barrier = pltpu.get_barrier_semaphore()
    peers = 0
    for dz in range(4):
        for dx in range(4):
            for dy in range(4):
                for dc in range(2):
                    if (dz and dx and dy) or not (dz or dx or dy or dc):
                        continue
                    peers += 1
                    pl.semaphore_signal(
                        barrier, 1, device_id=device(wrap4(z + dz), wrap4(x + dx), wrap4(y + dy), c ^ dc),
                        device_id_type=MESH,
                    )

    loads = [
        pltpu.make_async_copy(k_hbm, kx.at[pl.ds(128, 2048)], load_sem.at[0]),
        pltpu.make_async_copy(v_hbm, vx.at[pl.ds(128, 2048)], load_sem.at[1]),
        pltpu.make_async_copy(q_hbm, q, load_sem.at[2]),
        pltpu.make_async_copy(row_cos_hbm.at[pl.ds(ep * 32, 36)], row_cos, load_sem.at[3]),
        pltpu.make_async_copy(row_sin_hbm.at[pl.ds(ep * 32, 36)], row_sin, load_sem.at[4]),
        pltpu.make_async_copy(wg_hbm.at[0], wg, load_sem.at[5]),
        pltpu.make_async_copy(wu_hbm.at[0], wu, load_sem.at[6]),
        pltpu.make_async_copy(wd_hbm.at[0], wd, load_sem.at[7]),
        pltpu.make_async_copy(mix_hbm, mix, load_sem.at[8]),
    ]
    first_loads = [
        pltpu.make_async_copy(src, dst, load_sem.at[9 + n])
        for n, (src, dst) in enumerate(
            (
                (x_hbm, x_ref), (gain_hbm, gain_ref), (routes_hbm, routes_ref), (shares_hbm, shares_ref),
                (pairs_hbm, pairs_ref), (col_cos_hbm, col_cos_ref), (col_sin_hbm, col_sin_ref),
            )
        )
    ]
    for copy in first_loads + loads:
        copy.start()
    for copy in first_loads:
        copy.wait()

    values = x_ref[...].astype(F32)
    center = jnp.mean(values, axis=-1, keepdims=True)
    moved = values - center
    spread = jnp.mean(jnp.square(moved), axis=-1, keepdims=True)
    nrm[...] = (moved * lax.rsqrt(spread + NORM_EPS) * gain_ref[...]).astype(BF16)
    expert_of = lax.broadcasted_iota(jnp.int32, (128, 128), 0).astype(F32)
    routes = [routes_ref[k : k + 1, :].astype(F32) for k in range(4)]
    named = [(expert_of == routes[k]).astype(F32) for k in range(4)]
    named_any = named[0] + named[1] + named[2] + named[3]
    earlier = (
        lax.broadcasted_iota(jnp.int32, (128, 128), 0) < lax.broadcasted_iota(jnp.int32, (128, 128), 1)
    ).astype(BF16)
    before = dot(named_any.astype(BF16), earlier)
    core = c.astype(F32)
    for k in range(4):
        slot = jnp.sum(before * named[k], axis=0, keepdims=True)
        own_meta[k : k + 1, :] = routes[k] * 16.0 + core * 8.0 + slot
        own_meta[4 + k : 5 + k, :] = shares_ref[k : k + 1, :]

    pl.semaphore_wait(barrier, peers)

    def line_peer(axis, j, cc):
        if axis == 0:
            return device(z, x, j, cc)
        if axis == 1:
            return device(z, j, y, cc)
        return device(j, x, y, cc)

    line_pos = (y, x, z)

    def remote(src, dst, ssem, rsem, target):
        pltpu.make_async_remote_copy(
            src_ref=src, dst_ref=dst, send_sem=ssem, recv_sem=rsem, device_id=target, device_id_type=MESH
        ).start()

    def drain(ref, sem):
        pltpu.make_async_copy(ref, ref, sem).wait()

    line_steps = [(2, 0), (2, 1), (1, 0), (3, 0), (1, 1), (3, 1), (0, 1)]
    for axis in AXES:
        for step, dc in line_steps:
            j = wrap4(line_pos[axis] + step)
            remote(
                own_meta, metas.at[axis, line_pos[axis], :, pl.ds(aligned(c * 128), 128)],
                meta_send, meta_recv, line_peer(axis, j, c ^ dc),
            )
    for axis in (2, 1, 0):
        for step, dc in line_steps:
            j = wrap4(line_pos[axis] + step)
            cc = c ^ dc
            first = aligned(BASE[axis] + cc * COLS[axis])
            remote(
                nrm.at[:, pl.ds(first, COLS[axis])], ag[axis].at[line_pos[axis], c],
                ag_send.at[axis], ag_recv.at[axis], line_peer(axis, j, cc),
            )
    after, ahead = lax.rem(ep + 1, 16), lax.rem(ep + 15, 16)
    for n, (src, dst) in enumerate(((k_hbm, kx), (v_hbm, vx))):
        remote(
            src.at[pl.ds(1920, 128)], dst.at[pl.ds(0, 128)], halo_send.at[2 * n], halo_recv.at[2 * n], (after, tp)
        )
        remote(
            src.at[pl.ds(0, 128)], dst.at[pl.ds(2176, 128)], halo_send.at[2 * n + 1], halo_recv.at[2 * n + 1],
            (ahead, tp),
        )
    for axis in AXES:
        first = aligned(BASE[axis] + c * COLS[axis])
        ag[axis][line_pos[axis], c] = nrm[:, pl.ds(first, COLS[axis])]
        metas[axis, line_pos[axis], :, pl.ds(aligned(c * 128), 128)] = own_meta[...]

    def plane_expert(axis, e):
        if axis == 0:
            return (e // 2) * 8 + y * 2 + lax.rem(e, 2)
        if axis == 1:
            return (e // 8) * 32 + x * 8 + lax.rem(e, 8)
        return z * 32 + e

    self_at = ((z * 4 + x) * 2 + c, (z * 4 + y) * 2 + c, (x * 4 + y) * 2 + c)

    def place(axis):
        r = lax.broadcasted_iota(jnp.int32, (512, 256), 0)
        key = (plane_expert(axis, r // 16) * 16 + lax.rem(r, 16)).astype(F32)

        def one(j, carry):
            hit = key == metas[axis, j, 0:1, :]
            for k in range(1, 4):
                hit = hit | (key == metas[axis, j, k : k + 1, :])
            picks[axis, j] = hit.astype(F32).astype(BF16)
            return carry

        lax.fori_loop(0, 4, one, 0)

    def pack(axis):
        drain(ag[axis].at[:, :, pl.ds(0, 112), :], ag_recv.at[axis])
        for j in range(4):
            packed = dot(picks[axis, j], ag[axis][j].reshape(256, COLS[axis])).astype(BF16)
            pk[axis][:, j] = packed.reshape(32, 16, COLS[axis])

    def cols_of(axis, cc):
        return pl.ds(aligned(BASE[axis] + cc * COLS[axis]), COLS[axis])

    def back_cols(axis, cc):
        return pl.ds(aligned(BACK_BASE[axis] + cc * BACK_COLS[axis]), BACK_COLS[axis])

    def weigh_axis(axis):
        r = lax.broadcasted_iota(jnp.int32, (256, 512), 1)
        key = (plane_expert(axis, r // 16) * 16 + lax.rem(r, 16)).astype(F32)

        def weigh(j, carry):
            turned = jnp.transpose(metas[axis, j])
            share = jnp.zeros((256, 512), F32)
            for k in range(4):
                share += jnp.where(key == turned[:, k : k + 1], turned[:, 4 + k : 5 + k], 0.0)
            mixing[axis, j] = share.astype(BF16)
            return carry

        lax.fori_loop(0, 4, weigh, 0)

    for copy in loads[:5]:
        copy.wait()
    low = lax.rem(lax.broadcasted_iota(jnp.int32, (128, 128), 1), 128) < 64

    def turn_tables(g):
        cs = row_cos[pl.ds(g, 2)] + col_cos_ref[...][None]
        sn = row_sin[pl.ds(g, 2)] + col_sin_ref[...][None]
        return cs.reshape(128, 128), sn.reshape(128, 128)

    def turn_keys(b, carry):
        at = pl.ds(aligned(b * 128), 128)
        cs, sn = turn_tables(b * 2)
        kb = kx[at, :]
        turned = kb.astype(F32) * cs + dot(kb, pairs_ref[0:128, 0:128]) * sn
        krot[at, :] = turned.astype(BF16)
        kswap[at, :] = pltpu.roll(turned, 64, 1).astype(BF16)
        vswap[at, :] = pltpu.roll(vx[at, :].astype(F32), 64, 1).astype(BF16)
        return carry

    lax.fori_loop(1, 17, turn_keys, 0)
    i_at = lax.broadcasted_iota(jnp.int32, (256, 128), 0)
    i_at = lax.rem(i_at, 128)
    j_at = lax.broadcasted_iota(jnp.int32, (256, 128), 1)
    gap = j_at - i_at
    upper = lax.broadcasted_iota(jnp.int32, (256, 1), 0) < 128

    def attend(b):
        cs, sn = turn_tables(b * 2 + 2)
        cs = jnp.concatenate([cs, cs], axis=1)
        sn = jnp.concatenate([sn, sn], axis=1)
        qb = q[pl.ds(aligned(b * 128), 128), :]
        qr = (qb.astype(F32) * cs + dot(qb, pairs_ref[...]) * sn) * 0.125
        q01, q23 = qr[:, :128], qr[:, 128:]
        span = pl.ds(aligned(b * 128), 384)
        least = jnp.where((ep == 0) & (b == 0), 1000, 0)
        most = jnp.where((ep == 15) & (b == 15), -1000, 0)

        def pair(q_two, keys, vals, sink):
            s = lax.dot_general(
                q_two.astype(BF16), keys[span, :], (((1,), (1,)), ((), ())), preferred_element_type=F32
            )
            s0 = jnp.where(gap >= least, s[:, :128], -1e30)
            s1 = s[:, 128:256]
            s2 = jnp.where(gap <= most, s[:, 256:], -1e30)
            peak = jnp.maximum(
                jnp.max(jnp.maximum(jnp.maximum(s0, s1), s2), axis=1, keepdims=True), sink
            )
            e0, e1, e2 = jnp.exp(s0 - peak), jnp.exp(s1 - peak), jnp.exp(s2 - peak)
            total = jnp.sum(e0 + e1 + e2, axis=1, keepdims=True) + jnp.exp(sink - peak)
            inv = 1.0 / total
            p = jnp.concatenate([(e * inv).astype(BF16) for e in (e0, e1, e2)], axis=1)
            return dot(p, vals[span, :])

        oa = pair(
            jnp.concatenate([jnp.where(low, q01, 0.0), jnp.where(low, 0.0, q23)], axis=0), krot, vx,
            jnp.where(upper, sink_ref[0], sink_ref[3]),
        )
        ob = pair(
            jnp.concatenate([jnp.where(low, 0.0, q01), jnp.where(low, q23, 0.0)], axis=0), kswap, vswap,
            jnp.where(upper, sink_ref[1], sink_ref[2]),
        )
        out = jnp.concatenate(
            [jnp.where(low, oa[:128], ob[:128]), jnp.where(low, ob[128:], oa[128:])], axis=1
        )
        att[pl.ds(aligned(b * 128), 128), :] = out.astype(BF16)

    def attend_for(s, carry):
        t = lax.rem(tp + 1 + s, 8)

        def half(h, inner):
            attend(t * 2 + h)
            return inner

        lax.fori_loop(0, 2, half, 0)
        here = att.at[pl.ds(aligned(t * 256, 256), 256)]

        @pl.when(s < 7)
        def _():
            remote(here, att_in.at[:, pl.ds(aligned(tp * 256), 256)], att_send, att_recv, (ep, t))

        return carry

    drain(dummy, meta_recv)
    place(2)
    place(1)
    place(0)
    def send_rows(items):
        for axis, dz, *rest in items:
            if axis == 0:
                zt, xt, ct = wrap4(z + dz), wrap4(x + rest[0]), c ^ rest[1]
                src, dst = pk_y.at[(zt * 4 + xt) * 2 + ct, rest[2]], arr.at[z, x, rest[2], :, cols_of(0, c)]
                target = device(zt, xt, y, ct)
            elif axis == 1:
                zt, yt, ct = wrap4(z + dz), wrap4(y + rest[0]), c ^ rest[1]
                src, dst = pk_x.at[(zt * 4 + yt) * 2 + ct, rest[2]], arr.at[z, rest[2], y, :, cols_of(1, c)]
                target = device(zt, x, yt, ct)
            else:
                xt, yt, ct = wrap4(x + rest[0]), wrap4(y + rest[1]), c ^ rest[2]
                zs = wrap4(z + 4 - dz)
                src, dst = pk_z.at[(xt * 4 + yt) * 2 + ct, zs], arr.at[zs, x, y, :, cols_of(2, c)]
                target = device(z, xt, yt, ct)
            chunk = [n for n, steps in enumerate(CHUNKS) if dz in steps][0]
            remote(src, dst, pk_send.at[axis], row_recv.at[axis, chunk], target)

    pack(2)
    pack(1)
    send_rows(messages(0, (1, 2)))
    pack(0)
    send_rows(messages(0, (0,)))
    arr[:, x, y, :, cols_of(2, c)] = pk_z[self_at[2]]
    arr[z, :, y, :, cols_of(1, c)] = pk_x[self_at[1]]
    arr[z, x, :, :, cols_of(0, c)] = pk_y[self_at[0]]

    drain(kx.at[pl.ds(0, 128)], halo_recv.at[0])
    drain(kx.at[pl.ds(2176, 128)], halo_recv.at[1])
    drain(vx.at[pl.ds(0, 128)], halo_recv.at[2])
    drain(vx.at[pl.ds(2176, 128)], halo_recv.at[3])
    turn_keys(0, 0)
    turn_keys(17, 0)
    lax.fori_loop(0, 4, attend_for, 0)
    send_rows(messages(1, (0, 1, 2)))
    lax.fori_loop(4, 8, attend_for, 0)

    for copy in loads[5:8]:
        copy.wait()
    for chunk, steps in enumerate(CHUNKS):
        count = 8 * len(steps) - (0 in steps)
        drain(pk_y.at[pl.ds(0, count)], row_recv.at[0, chunk])
        drain(pk_x.at[pl.ds(0, count)], row_recv.at[1, chunk])
        drain(pk_z.at[pl.ds(0, 31), pl.ds(0, len(steps))], row_recv.at[2, chunk])
        sources = [wrap4(z + 4 - dz) for dz in steps]
        here = pl.ds(0, 256 * len(steps))

        def hidden(f, carry):
            at = pl.ds(aligned(f * 256, 256), 256)
            rows = jnp.concatenate([arr[zs].reshape(256, 2048) for zs in sources], axis=0)
            gate = jnp.minimum(dot(rows, wg[:, at]), CLAMP_LIMIT)
            lift = jnp.clip(dot(rows, wu[:, at]), -CLAMP_LIMIT, CLAMP_LIMIT)
            act[here, at] = ((lift + 1.0) * gate * jax.nn.sigmoid(GATE_SLOPE * gate)).astype(BF16)
            return carry

        lax.fori_loop(0, 4, hidden, 0)

        def down(f, carry):
            at = pl.ds(aligned(f * 256, 256), 256)
            res = dot(act[here, :], wd[:, at]).astype(BF16)
            for n, zs in enumerate(sources):
                prod[zs, :, :, :, at] = res[256 * n : 256 * n + 256].reshape(4, 4, 16, 256)
            return carry

        for kind in AXES:
            first = BACK_BASE[kind] // 256
            lax.fori_loop(first, first + BACK_COLS[kind] // 128, down, 0)
            for axis, dz, *rest in messages(chunk, (kind,)):
                zs = wrap4(z + 4 - dz)
                if axis == 0:
                    xt, ct = wrap4(x + rest[0]), c ^ rest[1]
                    src, dst = prod.at[zs, xt, rest[2], :, back_cols(0, ct)], ret_y.at[self_at[0], rest[2]]
                    target = device(zs, xt, y, ct)
                elif axis == 1:
                    yt, ct = wrap4(y + rest[0]), c ^ rest[1]
                    src, dst = prod.at[zs, rest[2], yt, :, back_cols(1, ct)], ret_x.at[self_at[1], rest[2]]
                    target = device(zs, x, yt, ct)
                else:
                    xt, yt, ct = wrap4(x + rest[0]), wrap4(y + rest[1]), c ^ rest[2]
                    src, dst = prod.at[zs, xt, yt, :, back_cols(2, ct)], ret_z.at[self_at[2], zs]
                    target = device(z, xt, yt, ct)
                remote(src, dst, ret_send.at[axis], ret_recv.at[axis], target)
        if 0 in steps:
            ret_y[self_at[0]] = prod[z, x, :, :, back_cols(0, c)]
            ret_x[self_at[1]] = prod[z, :, y, :, back_cols(1, c)]
        for zs in sources:
            ret_z[self_at[2], zs] = prod[zs, x, y, :, back_cols(2, c)]

    att_in[:, pl.ds(aligned(tp * 256), 256)] = att[pl.ds(aligned(tp * 256, 256), 256), :]
    for axis in AXES:
        weigh_axis(axis)

    loads[8].wait()
    drain(att_in.at[:, pl.ds(0, 1792)], att_recv)

    def project(f, carry):
        at = pl.ds(aligned(f * 256, 256), 256)
        mo_ref[:, at] = dot(att_in[...], mix[:, at]).astype(BF16)
        return carry

    lax.fori_loop(0, 8, project, 0)
    give_mixed = pltpu.make_async_copy(mo_ref, mo_hbm, give_sem.at[0])
    give_mixed.start()

    for axis in (0, 1, 2):
        drain(ret[axis].at[pl.ds(0, 31)], ret_recv.at[axis])
        for step in (2, 1, 3, 0):
            j = wrap4(line_pos[axis] + step)
            rows = ret[axis][:, j].reshape(512, BACK_COLS[axis])
            part = dot(mixing[axis, j], rows).astype(BF16)
            out[axis][j] = part.reshape(2, 128, BACK_COLS[axis])
            slot = (4 - step) % 4
            for dc in range(2):
                cc = c ^ dc
                if step or dc:
                    remote(
                        out[axis].at[j, cc], rs[axis].at[c, slot],
                        rs_send.at[axis], rs_recv.at[axis], line_peer(axis, j, cc),
                    )
        rs[axis][c, 0] = out[axis][line_pos[axis], c]
    for axis in (0, 1, 2):
        drain(rs[axis].at[:, :, pl.ds(0, 112), :], rs_recv.at[axis])
        for cc in range(2):
            parts = [rs[axis][cc, s].astype(F32) for s in range(4)]
            first = BACK_BASE[axis] + cc * BACK_COLS[axis]
            eo_ref[:, first : first + BACK_COLS[axis]] = (parts[0] + parts[1] + parts[2] + parts[3]).astype(BF16)

    give_sums = pltpu.make_async_copy(eo_ref, eo_hbm, give_sem.at[1])
    give_sums.start()
    drain(dummy, meta_send)
    drain(kx.at[pl.ds(0, 128)], halo_send.at[0])
    drain(kx.at[pl.ds(0, 128)], halo_send.at[1])
    drain(kx.at[pl.ds(0, 128)], halo_send.at[2])
    drain(kx.at[pl.ds(0, 128)], halo_send.at[3])
    drain(att_in.at[:, pl.ds(0, 1792)], att_send)
    for axis in AXES:
        drain(pk[axis].at[pl.ds(0, 31)], pk_send.at[axis])
        drain(ret[axis].at[pl.ds(0, 31)], ret_send.at[axis])
        drain(out[axis].at[:, :, pl.ds(0, 112), :], rs_send.at[axis])
        drain(ag[axis].at[:, :, pl.ds(0, 112), :], ag_send.at[axis])
    give_mixed.wait()
    give_sums.wait()


def body(
    queries, key_heads, value_heads, sink_logits, mix_weight, expert_input, norm_gain,
    routes, route_weights, gate_weight, up_weight, down_weight,
):
    row_cos, row_sin, col_cos, col_sin, pairs = rope_tables()
    hbm = pl.BlockSpec(memory_space=pl.ANY)
    dma = pltpu.SemaphoreType.DMA
    V = pltpu.VMEM
    scratch = [
        V((128, 2048), BF16), V((1, 2048), F32), V((4, 128), jnp.int32), V((4, 128), F32), V((256, 256), BF16),
        V((64, 128), F32), V((64, 128), F32), V((256, 2048), BF16), V((128, 2048), BF16), dma((2,)),
        V((2048, 256), BF16), V((2304, 128), BF16), V((2304, 128), BF16),
        V((2304, 128), BF16), V((2304, 128), BF16), V((2304, 128), BF16),
        V((2048, 256), BF16), V((256, 2048), BF16),
        V((36, 1, 128), F32), V((36, 1, 128), F32),
        V((2048, 2048), BF16), V((2048, 1024), BF16), V((2048, 1024), BF16), V((1024, 2048), BF16),
        V((128, 2048), BF16), V((3, 4, 8, 256), F32),
        *[V((4, 2, 128, n), BF16) for n in COLS],
        *[V((32, 4, 16, n), BF16) for n in COLS],
        V((4, 4, 4, 16, 2048), BF16), V((512, 1024), BF16), V((4, 4, 4, 16, 2048), BF16),
        *[V((32, 4, 16, n), BF16) for n in BACK_COLS],
        V((3, 4, 256, 512), BF16), V((3, 4, 512, 256), BF16),
        *[V((2, 4, 128, n), BF16) for n in BACK_COLS], *[V((4, 2, 128, n), BF16) for n in BACK_COLS],
        V((8, 128), F32), V((168, 128), F32),
        dma((16,)), dma((4,)), dma((4,)), dma, dma, dma((3,)), dma((3,)),
        dma((3,)), dma((3, len(CHUNKS))), dma, dma, dma((3,)), dma((3,)), dma((3,)), dma((3,)),
    ]
    mixed, summed = pl.pallas_call(
        kernel,
        out_shape=(jax.ShapeDtypeStruct((256, 2048), BF16), jax.ShapeDtypeStruct((128, 2048), BF16)),
        in_specs=[pl.BlockSpec(memory_space=pltpu.SMEM)] + [hbm] * 16,
        out_specs=(hbm, hbm),
        scratch_shapes=scratch,
        compiler_params=pltpu.CompilerParams(
            collective_id=0, has_side_effects=True, vmem_limit_bytes=67043328
        ),
        name="layer",
    )(
        sink_logits, expert_input, norm_gain.reshape(1, -1), routes.T, route_weights.T, jnp.asarray(pairs, BF16),
        jnp.asarray(col_cos), jnp.asarray(col_sin), jnp.asarray(row_cos), jnp.asarray(row_sin),
        queries, key_heads, value_heads, mix_weight, gate_weight, up_weight, down_weight,
    )
    return pl.pallas_call(
        hand_over,
        out_shape=(jax.ShapeDtypeStruct((256, 2048), BF16), jax.ShapeDtypeStruct((128, 2048), BF16)),
        in_specs=[hbm] * 2,
        out_specs=(hbm, hbm),
        scratch_shapes=[V((384, 2048), BF16), dma((3,)), dma((3,))],
        name="finish",
    )(mixed, summed)


def hand_over(mixed, summed, mixed_out, summed_out, held, in_sem, out_sem):
    parts = [(mixed, mixed_out, 0, 0), (mixed, mixed_out, 128, 128), (summed, summed_out, 0, 256)]
    takes, gives = [], []
    for n, (src, dst, first, at) in enumerate(parts):
        here = held.at[pl.ds(at, 128)]
        takes.append(pltpu.make_async_copy(src.at[pl.ds(first, 128)], here, in_sem.at[n]))
        gives.append(pltpu.make_async_copy(here, dst.at[pl.ds(first, 128)], out_sem.at[n]))
    for copy in takes:
        copy.start()
    for take, give in zip(takes, gives):
        take.wait()
        give.start()
    for copy in gives:
        copy.wait()


def solution(mesh):
    return jax.shard_map(
        body,
        mesh=mesh,
        in_specs=(
            P("ep", "tp"), P("ep", "tp"), P("ep", "tp"), P("tp"), P(), P(("ep", "tp"), None), P(),
            P(("ep", "tp"), None), P(("ep", "tp"), None), P(("ep", "tp"), None, None),
            P(("ep", "tp"), None, None), P(("ep", "tp"), None, None),
        ),
        out_specs=(P(("ep", "tp"), None), P(("ep", "tp"), None)),
        check_vma=False,
    )
```

```python
import random

import jax
import jax.numpy as jnp
import numpy as np
from jax import lax
from jax.experimental import pallas as pl
from jax.experimental.pallas import tpu as pltpu
from jax.sharding import PartitionSpec as P

MESH = pl.DeviceIdType.MESH
BF16 = jnp.bfloat16
F32 = jnp.float32
GRID_W = 64
ROPE_BASE = 10000.0
CLAMP_LIMIT = 7.0
GATE_SLOPE = 1.702
NORM_EPS = 1e-05
BASE = (0, 768, 1536)
COLS = (384, 384, 256)
BACK_BASE = (0, 768, 1536)
BACK_COLS = (384, 384, 256)
AXES = (0, 1, 2)
CHUNKS = ((1, 3), (2, 0))


def shuffled(items):
    return random.Random(1).sample(items, len(items))


def messages(chunk, kinds):
    pairs = [(a, b) for a in range(4) for b in range(2)]
    items = []
    for dz in CHUNKS[chunk]:
        for axis in (0, 1):
            if axis in kinds:
                items += [(axis, dz, d, dc, n) for d, dc in pairs if dz or d or dc for n in range(4)]
        if 2 in kinds:
            items += [(2, dz, dx, dy, dc) for dx in range(4) for dy, dc in pairs if dx or dy or dc]
    return shuffled(items)


def rope_tables():
    freqs = np.float32(ROPE_BASE) ** (-np.arange(0, 32, 2, dtype=np.float32) / np.float32(32))
    lane = np.arange(128)
    by_row = (lane % 64) < 32
    freq = freqs[lane % 16].astype(np.float32)
    rows = np.clip(np.arange(-2, 514), 0, None).astype(np.float32)
    cols = np.arange(64).astype(np.float32)
    row_angle = (rows[:, None] * freq).astype(np.float32).astype(np.float64)
    col_angle = (cols[:, None] * freq).astype(np.float32).astype(np.float64)
    row_cos = np.where(by_row, np.cos(row_angle), 0.0).astype(np.float32)[:, None, :]
    row_sin = np.where(by_row, np.sin(row_angle), 0.0).astype(np.float32)[:, None, :]
    col_cos = np.where(by_row, 0.0, np.cos(col_angle)).astype(np.float32)
    col_sin = np.where(by_row, 0.0, np.sin(col_angle)).astype(np.float32)
    pairs = np.zeros((256, 256), np.float32)
    for l in range(256):
        if l % 32 < 16:
            pairs[l + 16, l] = -1.0
        else:
            pairs[l - 16, l] = 1.0
    return row_cos, row_sin, col_cos, col_sin, pairs


def device(z, x, y, c):
    return (z * 4 + x, y * 2 + c)


def wrap4(v):
    return lax.rem(v, 4)


def aligned(v, n=128):
    return pl.multiple_of(v, n)


def dot(a, b):
    return jnp.dot(a, b, preferred_element_type=F32)


def kernel(
    sink_ref, x_hbm, gain_hbm, routes_hbm, shares_hbm, pairs_hbm, col_cos_hbm, col_sin_hbm,
    row_cos_hbm, row_sin_hbm, q_hbm, k_hbm, v_hbm, mix_hbm, wg_hbm, wu_hbm, wd_hbm,
    mo_hbm, eo_hbm,
    x_ref, gain_ref, routes_ref, shares_ref, pairs_ref, col_cos_ref, col_sin_ref, mo_ref, eo_ref, give_sem, q, kx, vx, krot, kswap, vswap, att, att_in, row_cos, row_sin, mix, wg, wu, wd,
    nrm, metas, ag_y, ag_x, ag_z, pk_y, pk_x, pk_z, arr, act, prod, ret_y, ret_x, ret_z,
    mixing, picks, rs_y, rs_x, rs_z, out_y, out_x, out_z, own_meta, dummy,
    load_sem, halo_send, halo_recv, meta_send, meta_recv, ag_send, ag_recv,
    pk_send, row_recv, att_send, att_recv, ret_send, ret_recv, rs_send, rs_recv,
):
    ep, tp = lax.axis_index("ep"), lax.axis_index("tp")
    z, x, y, c = ep // 4, lax.rem(ep, 4), tp // 2, lax.rem(tp, 2)
    ag, pk, ret, rs = (ag_y, ag_x, ag_z), (pk_y, pk_x, pk_z), (ret_y, ret_x, ret_z), (rs_y, rs_x, rs_z)
    out = (out_y, out_x, out_z)

    barrier = pltpu.get_barrier_semaphore()
    peers = 0
    for dz in range(4):
        for dx in range(4):
            for dy in range(4):
                for dc in range(2):
                    if (dz and dx and dy) or not (dz or dx or dy or dc):
                        continue
                    peers += 1
                    pl.semaphore_signal(
                        barrier, 1, device_id=device(wrap4(z + dz), wrap4(x + dx), wrap4(y + dy), c ^ dc),
                        device_id_type=MESH,
                    )

    loads = [
        pltpu.make_async_copy(k_hbm, kx.at[pl.ds(128, 2048)], load_sem.at[0]),
        pltpu.make_async_copy(v_hbm, vx.at[pl.ds(128, 2048)], load_sem.at[1]),
        pltpu.make_async_copy(q_hbm, q, load_sem.at[2]),
        pltpu.make_async_copy(row_cos_hbm.at[pl.ds(ep * 32, 36)], row_cos, load_sem.at[3]),
        pltpu.make_async_copy(row_sin_hbm.at[pl.ds(ep * 32, 36)], row_sin, load_sem.at[4]),
        pltpu.make_async_copy(wg_hbm.at[0], wg, load_sem.at[5]),
        pltpu.make_async_copy(wu_hbm.at[0], wu, load_sem.at[6]),
        pltpu.make_async_copy(wd_hbm.at[0], wd, load_sem.at[7]),
        pltpu.make_async_copy(mix_hbm, mix, load_sem.at[8]),
    ]
    first_loads = [
        pltpu.make_async_copy(src, dst, load_sem.at[9 + n])
        for n, (src, dst) in enumerate(
            (
                (x_hbm, x_ref), (gain_hbm, gain_ref), (routes_hbm, routes_ref), (shares_hbm, shares_ref),
                (pairs_hbm, pairs_ref), (col_cos_hbm, col_cos_ref), (col_sin_hbm, col_sin_ref),
            )
        )
    ]
    for copy in first_loads + loads:
        copy.start()
    for copy in first_loads:
        copy.wait()

    values = x_ref[...].astype(F32)
    center = jnp.mean(values, axis=-1, keepdims=True)
    moved = values - center
    spread = jnp.mean(jnp.square(moved), axis=-1, keepdims=True)
    nrm[...] = (moved * lax.rsqrt(spread + NORM_EPS) * gain_ref[...]).astype(BF16)
    expert_of = lax.broadcasted_iota(jnp.int32, (128, 128), 0).astype(F32)
    routes = [routes_ref[k : k + 1, :].astype(F32) for k in range(4)]
    named = [(expert_of == routes[k]).astype(F32) for k in range(4)]
    named_any = named[0] + named[1] + named[2] + named[3]
    earlier = (
        lax.broadcasted_iota(jnp.int32, (128, 128), 0) < lax.broadcasted_iota(jnp.int32, (128, 128), 1)
    ).astype(BF16)
    before = dot(named_any.astype(BF16), earlier)
    core = c.astype(F32)
    for k in range(4):
        slot = jnp.sum(before * named[k], axis=0, keepdims=True)
        own_meta[k : k + 1, :] = routes[k] * 16.0 + core * 8.0 + slot
        own_meta[4 + k : 5 + k, :] = shares_ref[k : k + 1, :]

    pl.semaphore_wait(barrier, peers)

    def line_peer(axis, j, cc):
        if axis == 0:
            return device(z, x, j, cc)
        if axis == 1:
            return device(z, j, y, cc)
        return device(j, x, y, cc)

    line_pos = (y, x, z)

    def remote(src, dst, ssem, rsem, target):
        pltpu.make_async_remote_copy(
            src_ref=src, dst_ref=dst, send_sem=ssem, recv_sem=rsem, device_id=target, device_id_type=MESH
        ).start()

    def drain(ref, sem):
        pltpu.make_async_copy(ref, ref, sem).wait()

    line_steps = [(2, 0), (2, 1), (1, 0), (3, 0), (1, 1), (3, 1), (0, 1)]
    for axis in AXES:
        for step, dc in line_steps:
            j = wrap4(line_pos[axis] + step)
            remote(
                own_meta, metas.at[axis, line_pos[axis], :, pl.ds(aligned(c * 128), 128)],
                meta_send, meta_recv, line_peer(axis, j, c ^ dc),
            )
    for axis in (2, 1, 0):
        for step, dc in line_steps:
            j = wrap4(line_pos[axis] + step)
            cc = c ^ dc
            first = aligned(BASE[axis] + cc * COLS[axis])
            remote(
                nrm.at[:, pl.ds(first, COLS[axis])], ag[axis].at[line_pos[axis], c],
                ag_send.at[axis], ag_recv.at[axis], line_peer(axis, j, cc),
            )
    after, ahead = lax.rem(ep + 1, 16), lax.rem(ep + 15, 16)
    for n, (src, dst) in enumerate(((k_hbm, kx), (v_hbm, vx))):
        remote(
            src.at[pl.ds(1920, 128)], dst.at[pl.ds(0, 128)], halo_send.at[2 * n], halo_recv.at[2 * n], (after, tp)
        )
        remote(
            src.at[pl.ds(0, 128)], dst.at[pl.ds(2176, 128)], halo_send.at[2 * n + 1], halo_recv.at[2 * n + 1],
            (ahead, tp),
        )
    for axis in AXES:
        first = aligned(BASE[axis] + c * COLS[axis])
        ag[axis][line_pos[axis], c] = nrm[:, pl.ds(first, COLS[axis])]
        metas[axis, line_pos[axis], :, pl.ds(aligned(c * 128), 128)] = own_meta[...]

    def plane_expert(axis, e):
        if axis == 0:
            return (e // 2) * 8 + y * 2 + lax.rem(e, 2)
        if axis == 1:
            return (e // 8) * 32 + x * 8 + lax.rem(e, 8)
        return z * 32 + e

    self_at = ((z * 4 + x) * 2 + c, (z * 4 + y) * 2 + c, (x * 4 + y) * 2 + c)

    def place(axis):
        r = lax.broadcasted_iota(jnp.int32, (512, 256), 0)
        key = (plane_expert(axis, r // 16) * 16 + lax.rem(r, 16)).astype(F32)

        def one(j, carry):
            hit = key == metas[axis, j, 0:1, :]
            for k in range(1, 4):
                hit = hit | (key == metas[axis, j, k : k + 1, :])
            picks[axis, j] = hit.astype(F32).astype(BF16)
            return carry

        lax.fori_loop(0, 4, one, 0)

    def pack(axis):
        drain(ag[axis].at[:, :, pl.ds(0, 112), :], ag_recv.at[axis])
        for j in range(4):
            packed = dot(picks[axis, j], ag[axis][j].reshape(256, COLS[axis])).astype(BF16)
            pk[axis][:, j] = packed.reshape(32, 16, COLS[axis])

    def cols_of(axis, cc):
        return pl.ds(aligned(BASE[axis] + cc * COLS[axis]), COLS[axis])

    def back_cols(axis, cc):
        return pl.ds(aligned(BACK_BASE[axis] + cc * BACK_COLS[axis]), BACK_COLS[axis])

    def weigh_axis(axis):
        r = lax.broadcasted_iota(jnp.int32, (256, 512), 1)
        key = (plane_expert(axis, r // 16) * 16 + lax.rem(r, 16)).astype(F32)

        def weigh(j, carry):
            turned = jnp.transpose(metas[axis, j])
            share = jnp.zeros((256, 512), F32)
            for k in range(4):
                share += jnp.where(key == turned[:, k : k + 1], turned[:, 4 + k : 5 + k], 0.0)
            mixing[axis, j] = share.astype(BF16)
            return carry

        lax.fori_loop(0, 4, weigh, 0)

    for copy in loads[:5]:
        copy.wait()
    low = lax.rem(lax.broadcasted_iota(jnp.int32, (128, 128), 1), 128) < 64

    def turn_tables(g):
        cs = row_cos[pl.ds(g, 2)] + col_cos_ref[...][None]
        sn = row_sin[pl.ds(g, 2)] + col_sin_ref[...][None]
        return cs.reshape(128, 128), sn.reshape(128, 128)

    def turn_keys(b, carry):
        at = pl.ds(aligned(b * 128), 128)
        cs, sn = turn_tables(b * 2)
        kb = kx[at, :]
        turned = kb.astype(F32) * cs + dot(kb, pairs_ref[0:128, 0:128]) * sn
        krot[at, :] = turned.astype(BF16)
        kswap[at, :] = pltpu.roll(turned, 64, 1).astype(BF16)
        vswap[at, :] = pltpu.roll(vx[at, :].astype(F32), 64, 1).astype(BF16)
        return carry

    lax.fori_loop(1, 17, turn_keys, 0)
    i_at = lax.broadcasted_iota(jnp.int32, (256, 128), 0)
    i_at = lax.rem(i_at, 128)
    j_at = lax.broadcasted_iota(jnp.int32, (256, 128), 1)
    gap = j_at - i_at
    upper = lax.broadcasted_iota(jnp.int32, (256, 1), 0) < 128

    def attend(b):
        cs, sn = turn_tables(b * 2 + 2)
        cs = jnp.concatenate([cs, cs], axis=1)
        sn = jnp.concatenate([sn, sn], axis=1)
        qb = q[pl.ds(aligned(b * 128), 128), :]
        qr = (qb.astype(F32) * cs + dot(qb, pairs_ref[...]) * sn) * 0.125
        q01, q23 = qr[:, :128], qr[:, 128:]
        span = pl.ds(aligned(b * 128), 384)
        least = jnp.where((ep == 0) & (b == 0), 1000, 0)
        most = jnp.where((ep == 15) & (b == 15), -1000, 0)

        def pair(q_two, keys, vals, sink):
            s = lax.dot_general(
                q_two.astype(BF16), keys[span, :], (((1,), (1,)), ((), ())), preferred_element_type=F32
            )
            s0 = jnp.where(gap >= least, s[:, :128], -1e30)
            s1 = s[:, 128:256]
            s2 = jnp.where(gap <= most, s[:, 256:], -1e30)
            peak = jnp.maximum(
                jnp.max(jnp.maximum(jnp.maximum(s0, s1), s2), axis=1, keepdims=True), sink
            )
            e0, e1, e2 = jnp.exp(s0 - peak), jnp.exp(s1 - peak), jnp.exp(s2 - peak)
            total = jnp.sum(e0 + e1 + e2, axis=1, keepdims=True) + jnp.exp(sink - peak)
            inv = 1.0 / total
            p = jnp.concatenate([(e * inv).astype(BF16) for e in (e0, e1, e2)], axis=1)
            return dot(p, vals[span, :])

        oa = pair(
            jnp.concatenate([jnp.where(low, q01, 0.0), jnp.where(low, 0.0, q23)], axis=0), krot, vx,
            jnp.where(upper, sink_ref[0], sink_ref[3]),
        )
        ob = pair(
            jnp.concatenate([jnp.where(low, 0.0, q01), jnp.where(low, q23, 0.0)], axis=0), kswap, vswap,
            jnp.where(upper, sink_ref[1], sink_ref[2]),
        )
        out = jnp.concatenate(
            [jnp.where(low, oa[:128], ob[:128]), jnp.where(low, ob[128:], oa[128:])], axis=1
        )
        att[pl.ds(aligned(b * 128), 128), :] = out.astype(BF16)

    def attend_for(s, carry):
        t = lax.rem(tp + 1 + s, 8)

        def half(h, inner):
            attend(t * 2 + h)
            return inner

        lax.fori_loop(0, 2, half, 0)
        here = att.at[pl.ds(aligned(t * 256, 256), 256)]

        @pl.when(s < 7)
        def _():
            remote(here, att_in.at[:, pl.ds(aligned(tp * 256), 256)], att_send, att_recv, (ep, t))

        return carry

    drain(dummy, meta_recv)
    place(2)
    place(1)
    place(0)
    def send_rows(items):
        for axis, dz, *rest in items:
            if axis == 0:
                zt, xt, ct = wrap4(z + dz), wrap4(x + rest[0]), c ^ rest[1]
                src, dst = pk_y.at[(zt * 4 + xt) * 2 + ct, rest[2]], arr.at[z, x, rest[2], :, cols_of(0, c)]
                target = device(zt, xt, y, ct)
            elif axis == 1:
                zt, yt, ct = wrap4(z + dz), wrap4(y + rest[0]), c ^ rest[1]
                src, dst = pk_x.at[(zt * 4 + yt) * 2 + ct, rest[2]], arr.at[z, rest[2], y, :, cols_of(1, c)]
                target = device(zt, x, yt, ct)
            else:
                xt, yt, ct = wrap4(x + rest[0]), wrap4(y + rest[1]), c ^ rest[2]
                zs = wrap4(z + 4 - dz)
                src, dst = pk_z.at[(xt * 4 + yt) * 2 + ct, zs], arr.at[zs, x, y, :, cols_of(2, c)]
                target = device(z, xt, yt, ct)
            chunk = [n for n, steps in enumerate(CHUNKS) if dz in steps][0]
            remote(src, dst, pk_send.at[axis], row_recv.at[axis, chunk], target)

    pack(2)
    pack(1)
    send_rows(messages(0, (1, 2)))
    pack(0)
    send_rows(messages(0, (0,)))
    arr[:, x, y, :, cols_of(2, c)] = pk_z[self_at[2]]
    arr[z, :, y, :, cols_of(1, c)] = pk_x[self_at[1]]
    arr[z, x, :, :, cols_of(0, c)] = pk_y[self_at[0]]

    drain(kx.at[pl.ds(0, 128)], halo_recv.at[0])
    drain(kx.at[pl.ds(2176, 128)], halo_recv.at[1])
    drain(vx.at[pl.ds(0, 128)], halo_recv.at[2])
    drain(vx.at[pl.ds(2176, 128)], halo_recv.at[3])
    turn_keys(0, 0)
    turn_keys(17, 0)
    lax.fori_loop(0, 3, attend_for, 0)
    send_rows(messages(1, (0, 1, 2)))
    lax.fori_loop(3, 6, attend_for, 0)

    for copy in loads[5:8]:
        copy.wait()
    for chunk, steps in enumerate(CHUNKS):
        count = 8 * len(steps) - (0 in steps)
        drain(pk_y.at[pl.ds(0, count)], row_recv.at[0, chunk])
        drain(pk_x.at[pl.ds(0, count)], row_recv.at[1, chunk])
        drain(pk_z.at[pl.ds(0, 31), pl.ds(0, len(steps))], row_recv.at[2, chunk])
        sources = [wrap4(z + 4 - dz) for dz in steps]
        here = pl.ds(0, 256 * len(steps))

        def hidden(f, carry):
            at = pl.ds(aligned(f * 256, 256), 256)
            rows = jnp.concatenate([arr[zs].reshape(256, 2048) for zs in sources], axis=0)
            gate = jnp.minimum(dot(rows, wg[:, at]), CLAMP_LIMIT)
            lift = jnp.clip(dot(rows, wu[:, at]), -CLAMP_LIMIT, CLAMP_LIMIT)
            act[here, at] = ((lift + 1.0) * gate * jax.nn.sigmoid(GATE_SLOPE * gate)).astype(BF16)
            return carry

        lax.fori_loop(0, 4, hidden, 0)

        def down(f, carry):
            at = pl.ds(aligned(f * 256, 256), 256)
            res = dot(act[here, :], wd[:, at]).astype(BF16)
            for n, zs in enumerate(sources):
                prod[zs, :, :, :, at] = res[256 * n : 256 * n + 256].reshape(4, 4, 16, 256)
            return carry

        for kind in AXES:
            first = BACK_BASE[kind] // 256
            lax.fori_loop(first, first + BACK_COLS[kind] // 128, down, 0)
            for axis, dz, *rest in messages(chunk, (kind,)):
                zs = wrap4(z + 4 - dz)
                if axis == 0:
                    xt, ct = wrap4(x + rest[0]), c ^ rest[1]
                    src, dst = prod.at[zs, xt, rest[2], :, back_cols(0, ct)], ret_y.at[self_at[0], rest[2]]
                    target = device(zs, xt, y, ct)
                elif axis == 1:
                    yt, ct = wrap4(y + rest[0]), c ^ rest[1]
                    src, dst = prod.at[zs, rest[2], yt, :, back_cols(1, ct)], ret_x.at[self_at[1], rest[2]]
                    target = device(zs, x, yt, ct)
                else:
                    xt, yt, ct = wrap4(x + rest[0]), wrap4(y + rest[1]), c ^ rest[2]
                    src, dst = prod.at[zs, xt, yt, :, back_cols(2, ct)], ret_z.at[self_at[2], zs]
                    target = device(z, xt, yt, ct)
                remote(src, dst, ret_send.at[axis], ret_recv.at[axis], target)
        if 0 in steps:
            ret_y[self_at[0]] = prod[z, x, :, :, back_cols(0, c)]
            ret_x[self_at[1]] = prod[z, :, y, :, back_cols(1, c)]
        if chunk == 0:
            lax.fori_loop(6, 8, attend_for, 0)
        for zs in sources:
            ret_z[self_at[2], zs] = prod[zs, x, y, :, back_cols(2, c)]

    att_in[:, pl.ds(aligned(tp * 256), 256)] = att[pl.ds(aligned(tp * 256, 256), 256), :]
    for axis in AXES:
        weigh_axis(axis)

    loads[8].wait()
    drain(att_in.at[:, pl.ds(0, 1792)], att_recv)

    def project(f, carry):
        at = pl.ds(aligned(f * 256, 256), 256)
        mo_ref[:, at] = dot(att_in[...], mix[:, at]).astype(BF16)
        return carry

    lax.fori_loop(0, 8, project, 0)
    give_mixed = pltpu.make_async_copy(mo_ref, mo_hbm, give_sem.at[0])
    give_mixed.start()

    for axis in (0, 1, 2):
        drain(ret[axis].at[pl.ds(0, 31)], ret_recv.at[axis])
        for step in (2, 1, 3, 0):
            j = wrap4(line_pos[axis] + step)
            rows = ret[axis][:, j].reshape(512, BACK_COLS[axis])
            part = dot(mixing[axis, j], rows).astype(BF16)
            out[axis][j] = part.reshape(2, 128, BACK_COLS[axis])
            slot = (4 - step) % 4
            for dc in range(2):
                cc = c ^ dc
                if step or dc:
                    remote(
                        out[axis].at[j, cc], rs[axis].at[c, slot],
                        rs_send.at[axis], rs_recv.at[axis], line_peer(axis, j, cc),
                    )
        rs[axis][c, 0] = out[axis][line_pos[axis], c]
    for axis in (0, 1, 2):
        drain(rs[axis].at[:, :, pl.ds(0, 112), :], rs_recv.at[axis])
        for cc in range(2):
            parts = [rs[axis][cc, s].astype(F32) for s in range(4)]
            first = BACK_BASE[axis] + cc * BACK_COLS[axis]
            eo_ref[:, first : first + BACK_COLS[axis]] = (parts[0] + parts[1] + parts[2] + parts[3]).astype(BF16)

    give_sums = pltpu.make_async_copy(eo_ref, eo_hbm, give_sem.at[1])
    give_sums.start()
    drain(dummy, meta_send)
    drain(kx.at[pl.ds(0, 128)], halo_send.at[0])
    drain(kx.at[pl.ds(0, 128)], halo_send.at[1])
    drain(kx.at[pl.ds(0, 128)], halo_send.at[2])
    drain(kx.at[pl.ds(0, 128)], halo_send.at[3])
    drain(att_in.at[:, pl.ds(0, 1792)], att_send)
    for axis in AXES:
        drain(pk[axis].at[pl.ds(0, 31)], pk_send.at[axis])
        drain(ret[axis].at[pl.ds(0, 31)], ret_send.at[axis])
        drain(out[axis].at[:, :, pl.ds(0, 112), :], rs_send.at[axis])
        drain(ag[axis].at[:, :, pl.ds(0, 112), :], ag_send.at[axis])
    give_mixed.wait()
    give_sums.wait()


def body(
    queries, key_heads, value_heads, sink_logits, mix_weight, expert_input, norm_gain,
    routes, route_weights, gate_weight, up_weight, down_weight,
):
    row_cos, row_sin, col_cos, col_sin, pairs = rope_tables()
    hbm = pl.BlockSpec(memory_space=pl.ANY)
    dma = pltpu.SemaphoreType.DMA
    V = pltpu.VMEM
    scratch = [
        V((128, 2048), BF16), V((1, 2048), F32), V((4, 128), jnp.int32), V((4, 128), F32), V((256, 256), BF16),
        V((64, 128), F32), V((64, 128), F32), V((256, 2048), BF16), V((128, 2048), BF16), dma((2,)),
        V((2048, 256), BF16), V((2304, 128), BF16), V((2304, 128), BF16),
        V((2304, 128), BF16), V((2304, 128), BF16), V((2304, 128), BF16),
        V((2048, 256), BF16), V((256, 2048), BF16),
        V((36, 1, 128), F32), V((36, 1, 128), F32),
        V((2048, 2048), BF16), V((2048, 1024), BF16), V((2048, 1024), BF16), V((1024, 2048), BF16),
        V((128, 2048), BF16), V((3, 4, 8, 256), F32),
        *[V((4, 2, 128, n), BF16) for n in COLS],
        *[V((32, 4, 16, n), BF16) for n in COLS],
        V((4, 4, 4, 16, 2048), BF16), V((512, 1024), BF16), V((4, 4, 4, 16, 2048), BF16),
        *[V((32, 4, 16, n), BF16) for n in BACK_COLS],
        V((3, 4, 256, 512), BF16), V((3, 4, 512, 256), BF16),
        *[V((2, 4, 128, n), BF16) for n in BACK_COLS], *[V((4, 2, 128, n), BF16) for n in BACK_COLS],
        V((8, 128), F32), V((168, 128), F32),
        dma((16,)), dma((4,)), dma((4,)), dma, dma, dma((3,)), dma((3,)),
        dma((3,)), dma((3, len(CHUNKS))), dma, dma, dma((3,)), dma((3,)), dma((3,)), dma((3,)),
    ]
    mixed, summed = pl.pallas_call(
        kernel,
        out_shape=(jax.ShapeDtypeStruct((256, 2048), BF16), jax.ShapeDtypeStruct((128, 2048), BF16)),
        in_specs=[pl.BlockSpec(memory_space=pltpu.SMEM)] + [hbm] * 16,
        out_specs=(hbm, hbm),
        scratch_shapes=scratch,
        compiler_params=pltpu.CompilerParams(
            collective_id=0, has_side_effects=True, vmem_limit_bytes=67043328
        ),
        name="layer",
    )(
        sink_logits, expert_input, norm_gain.reshape(1, -1), routes.T, route_weights.T, jnp.asarray(pairs, BF16),
        jnp.asarray(col_cos), jnp.asarray(col_sin), jnp.asarray(row_cos), jnp.asarray(row_sin),
        queries, key_heads, value_heads, mix_weight, gate_weight, up_weight, down_weight,
    )
    return pl.pallas_call(
        hand_over,
        out_shape=(jax.ShapeDtypeStruct((256, 2048), BF16), jax.ShapeDtypeStruct((128, 2048), BF16)),
        in_specs=[hbm] * 2,
        out_specs=(hbm, hbm),
        scratch_shapes=[V((384, 2048), BF16), dma((3,)), dma((3,))],
        name="finish",
    )(mixed, summed)


def hand_over(mixed, summed, mixed_out, summed_out, held, in_sem, out_sem):
    parts = [(mixed, mixed_out, 0, 0), (mixed, mixed_out, 128, 128), (summed, summed_out, 0, 256)]
    takes, gives = [], []
    for n, (src, dst, first, at) in enumerate(parts):
        here = held.at[pl.ds(at, 128)]
        takes.append(pltpu.make_async_copy(src.at[pl.ds(first, 128)], here, in_sem.at[n]))
        gives.append(pltpu.make_async_copy(here, dst.at[pl.ds(first, 128)], out_sem.at[n]))
    for copy in takes:
        copy.start()
    for take, give in zip(takes, gives):
        take.wait()
        give.start()
    for copy in gives:
        copy.wait()


def solution(mesh):
    return jax.shard_map(
        body,
        mesh=mesh,
        in_specs=(
            P("ep", "tp"), P("ep", "tp"), P("ep", "tp"), P("tp"), P(), P(("ep", "tp"), None), P(),
            P(("ep", "tp"), None), P(("ep", "tp"), None), P(("ep", "tp"), None, None),
            P(("ep", "tp"), None, None), P(("ep", "tp"), None, None),
        ),
        out_specs=(P(("ep", "tp"), None), P(("ep", "tp"), None)),
        check_vma=False,
    )
```
